32 devices in a mesh: sp: 8 (over z, x), tp: 4 (over y, core).
Axes of the slice: x: 2, y: 2, z: 4, core: 2. Of those that a mesh axis runs over, the one named last changes fastest.
Arguments:
- readout_query_vectors: bfloat16 [2048, 2048], P('sp', 'tp'), may hold values from -6 to 6
- attention_key_vectors: bfloat16 [2048, 2048], P('sp', 'tp'), may hold values from -6 to 6
- attention_content_vectors: bfloat16 [2048, 2048], P('sp', 'tp'), may hold values from -6 to 6
- step_size_preactivation: bfloat16 [2048, 2048], P('sp', 'tp'), may hold values from -16 to 8
- forgetting_preactivation: float32 [2048, 2048], P('sp', 'tp'), may hold values from -22 to 3
- extra_forgetting_bias: float32 [2048, 32], P('sp', 'tp'), may hold values from -0.7 to 0
- subspace_normalizer_gain: float32 [2048], P('tp'), may hold values from 0.1 to 1.9
- skip_connection_stream: bfloat16 [2048, 2048], P('sp'), may hold values from -40 to 40
- blender_projection_matrix: bfloat16 [2048, 2048], P('tp'), may hold values from -0.125 to 0.125
- specialist_prenormal_gain: float32 [2048], replicated, may hold values from 0.1 to 1.9
- cluster_router_chance: float32 [2048], P('sp'), may hold values from 0.4 to 1
- specialist_chance_within_cluster: float32 [2048, 2], P('sp'), may hold values from 0.1 to 1
- chosen_specialist_ids: int32 [2048, 2], P('sp'), may hold values from 0 to 7, all different within a row; in each aligned block of 256 rows (0 to 255, 256 to 511, ...) at most 128 rows name the same one
- specialist_switch_matrix: bfloat16 [8, 2048, 2048], P('sp', None, 'tp'), may hold values from -0.125 to 0.125
- specialist_expansion_matrix: bfloat16 [8, 2048, 2048], P('sp', None, 'tp'), may hold values from -0.125 to 0.125
- specialist_contraction_matrix: bfloat16 [8, 2048, 2048], P('sp', 'tp'), may hold values from -0.375 to 0.375
Outputs:
- layer_out: bfloat16 [2048, 2048], P('sp')
The draws below stay inside these ranges and needn't reach their ends.
Inputs may be any that keep to these rules, and one draw needn't show every extreme that they name: `chosen_specialist_ids`: in each aligned block of 256 rows every expert is named at most 128 times.
All inputs are finite; a program needn't handle non-finite values.
Results may differ from the reference program's by a relative error of at most 0.022.
Values may be sent and summed in bfloat16 or wider, within the bound.
A program may use at most 64 MiB of HBM per device.

```python
import math
import jax
import jax.numpy as jnp
import numpy as np
from jax import lax

D = 2048
HEAD_DIM = 64
HEAD_TOTAL = 32
FF = 2048
TOP = 2
TOK_DEV = 256
TOKEN_TOTAL = 2048
EXPERTS = 8
CAP = 128
N_SP = 8
N_TP = 4


def slow_heads(key):
    chance = jax.random.uniform(jax.random.fold_in(key, 11), (HEAD_TOTAL,))
    return chance < 0.5


def draw_forgetting_preactivation(key, part):
    slow = slow_heads(key)
    head_base = jnp.where(slow, jnp.log(0.7 / TOKEN_TOTAL) + 0.5, -3.2)
    first_key = jax.random.fold_in(key, 3)
    second_key = jax.random.fold_in(key, 4)
    third_key = jax.random.fold_in(key, 5)
    jitter = 0.3 * jax.random.normal(first_key, (HEAD_TOTAL,))
    offset = jax.random.uniform(second_key, (TOKEN_TOTAL // 64, HEAD_TOTAL), minval=-0.7, maxval=0.7)
    offset = jnp.repeat(offset, 64, axis=0)
    noise_part = 0.6 * jax.random.normal(third_key, (TOKEN_TOTAL, HEAD_TOTAL, HEAD_DIM))
    result = head_base[None, :, None] + jitter[None, :, None] + offset[:, :, None] + noise_part
    return result.reshape(TOKEN_TOTAL, HEAD_TOTAL * HEAD_DIM).astype(jnp.float32)


def draw_step_size_preactivation(key, part):
    slow = slow_heads(key)
    head_base = jnp.where(slow, jnp.log(0.25 * HEAD_DIM / TOKEN_TOTAL), 0.0)
    noise_key = jax.random.fold_in(key, 6)
    noise_part = 0.8 * jax.random.normal(noise_key, (TOKEN_TOTAL, HEAD_TOTAL, HEAD_DIM))
    result = head_base[None, :, None] + noise_part
    return result.reshape(TOKEN_TOTAL, HEAD_TOTAL * HEAD_DIM).astype(jnp.bfloat16)


def draw_extra_forgetting_bias(key, part):
    spike_positions = jax.random.randint(jax.random.fold_in(key, 1), (8,), 0, TOKEN_TOTAL)
    spiked_values = jnp.any(jnp.arange(TOKEN_TOTAL)[:, None] == spike_positions[None, :], axis=1)
    spike_depth = jnp.log(jax.random.uniform(jax.random.fold_in(key, 2), (TOKEN_TOTAL, HEAD_TOTAL), minval=0.5, maxval=0.8))
    return jnp.where(spiked_values[:, None], spike_depth, 0.0).astype(jnp.float32)


def draw_skip_connection_stream(key, part):
    column = jnp.exp(jax.random.uniform(jax.random.fold_in(key, 1), (D,), minval=-0.6, maxval=0.6))
    result = jax.random.normal(jax.random.fold_in(key, 2), (TOKEN_TOTAL, D)) * column
    return result.astype(jnp.bfloat16)


def steps_of(key, extent, shards, low, top_value):
    level, own = 1.0, jax.random.fold_in(key, 6)
    for position, parts in shards:
        steps = jnp.exp(jax.random.uniform(jax.random.fold_in(own, position), (parts,), jnp.float32, low / len(shards), top_value / len(shards)))
        level = level * jnp.repeat(steps, extent[position] // parts).reshape([-1 if axis == position else 1 for axis in range(len(extent))])
    return level


def assign_block(stream_key, own, number, rows, number_of, top, limit, skew):
    order = jax.random.permutation(stream_key, number_of)
    heavy_load, common = portions_of(number_of, rows * top, limit, skew, True), portions_of(number_of, rows * top, limit, skew, False)
    places = jnp.arange(number_of)

    def named(sizes, rotation):
        used = int((sizes > 0).sum())
        fixed = max(1, used // 4)
        moved = fixed + (places - fixed + rotation * (used - fixed)) % max(1, number_of - fixed)
        return jnp.zeros((number_of,), jnp.int32).at[order[jnp.where(places < fixed, places, moved)]].set(jnp.asarray(sizes, jnp.int32))

    sizes = jnp.where(number % 4 == 0, named(heavy_load, number // 4), named(common, number - number // 4 - 1))
    mixed = jax.random.permutation(jax.random.fold_in(own, 3), number_of)
    source_of, receiver = mixed[0:number_of // 2 * 2:2], mixed[1:number_of // 2 * 2:2]
    margin = jnp.minimum(sizes[source_of] - 1, limit - sizes[receiver]) // 2
    margin = jnp.where((source_of == order[0]) | (receiver == order[0]) | (sizes[receiver] == 0), 0, jnp.maximum(margin, 0))
    moved = jax.random.randint(jax.random.fold_in(own, 4), (number_of // 2,), 0, 1 << 20) % (margin + 1)
    sizes = sizes.at[source_of].add(-moved).at[receiver].add(moved)
    members = jnp.searchsorted(jnp.cumsum(sizes), jnp.arange(rows * top), side="right").astype(jnp.int32)
    grid = members.reshape(top, rows).T
    grid = grid[jax.random.permutation(jax.random.fold_in(own, 1), rows)]
    rotation = jax.random.randint(jax.random.fold_in(own, 2), (rows, 1), 0, top)
    return jnp.take_along_axis(grid, (jnp.arange(top)[None, :] + rotation) % top, axis=1)


def portions_of(number_of, total, most, skew, full):
    loads = [(1 << 20) // math.isqrt(standing ** skew) + 1 for standing in range(1, number_of + 1)]
    largest = most if full else min(most, max(-(-total // number_of), total * loads[0] // sum(loads)))
    least = 1 if total - largest >= number_of - 1 else 0
    holding, rest = [largest] + [least] * (number_of - 1), total - largest - least * (number_of - 1)
    while rest > 0:
        free = [i for i in range(1, number_of) if holding[i] < largest] or [i for i in range(1, number_of) if holding[i] < most]
        pool, remaining = sum([loads[i] for i in free]), rest
        for i in free:
            addition = min(most - holding[i], max(1, remaining * loads[i] // pool), rest)
            holding[i] = holding[i] + addition
            rest = rest - addition
    return np.array(holding)


def centred(rng, extent, deviation, most, pieces=(), held_as=jnp.bfloat16):
    gain = steps_of(rng, extent, pieces, -0.22, 0.18) if pieces else 1.0
    values = jax.random.normal(rng, extent, jnp.float32) * deviation * gain
    return jnp.minimum(jnp.maximum(values, -most), most).astype(held_as)


def setup_inputs(seed: int = 0) -> dict:
    key_of = jax.random.split(jax.random.key(seed), 17)
    readout_query_vectors = centred(key_of[0], (TOKEN_TOTAL, D), 1.0, 6.0, ((0, 8), (1, 4)))
    attention_key_vectors = centred(key_of[1], (TOKEN_TOTAL, D), 1.0, 6.0, ((0, 8), (1, 4)))
    attention_content_vectors = centred(key_of[2], (TOKEN_TOTAL, D), 1.0, 6.0, ((0, 8), (1, 4)))
    step_size_preactivation = draw_step_size_preactivation(jax.random.fold_in(key_of[16], 71), 0)
    forgetting_preactivation = draw_forgetting_preactivation(jax.random.fold_in(key_of[16], 71), 0)
    extra_forgetting_bias = draw_extra_forgetting_bias(jax.random.fold_in(key_of[16], 71), 0)
    subspace_normalizer_gain = jnp.clip(1.0 + 0.18 * jax.random.normal(key_of[6], (D,), jnp.float32), 0.1, 1.9)
    skip_connection_stream = draw_skip_connection_stream(jax.random.fold_in(key_of[16], 71), 0)
    blender_projection_matrix = centred(key_of[8], (D, D), D ** -0.5, 0.125, ((0, 4),))
    specialist_prenormal_gain = jnp.clip(1.0 + 0.18 * jax.random.normal(key_of[9], (D,), jnp.float32), 0.1, 1.9)
    cluster_router_chance = jnp.clip(0.4 + 0.6 * jax.random.uniform(key_of[10], (TOKEN_TOTAL,), jnp.float32) ** steps_of(key_of[10], (TOKEN_TOTAL,), ((0, 8),), -0.2, 0.2), 0.4, 1.0)
    specialist_chance_within_cluster = jnp.clip(0.1 + 0.9 * jax.random.uniform(key_of[11], (TOKEN_TOTAL, TOP), jnp.float32) ** steps_of(key_of[11], (TOKEN_TOTAL, TOP), ((0, 8),), -0.2, 0.2), 0.1, 1.0)
    chosen_specialist_ids_keys = jax.random.split(jax.random.fold_in(key_of[12], 1), TOKEN_TOTAL // TOK_DEV)
    chosen_specialist_ids_turns = jax.random.permutation(jax.random.fold_in(key_of[12], 3), TOKEN_TOTAL // TOK_DEV)
    chosen_specialist_ids = jax.vmap(lambda own, number: assign_block(jax.random.fold_in(key_of[12], 2), own, number, TOK_DEV, EXPERTS, TOP, CAP, 1))(chosen_specialist_ids_keys, chosen_specialist_ids_turns).reshape((TOKEN_TOTAL, TOP))
    specialist_switch_matrix = centred(key_of[13], (EXPERTS, D, FF), D ** -0.5, 0.125, ((0, 8), (2, 4)))
    specialist_expansion_matrix = centred(key_of[14], (EXPERTS, D, FF), D ** -0.5, 0.125, ((0, 8), (2, 4)))
    specialist_contraction_matrix = centred(key_of[15], (EXPERTS, FF, D), (FF // 8) ** -0.5, 0.375, ((0, 8), (1, 4)))
    return dict(readout_query_vectors=readout_query_vectors, attention_key_vectors=attention_key_vectors, attention_content_vectors=attention_content_vectors, step_size_preactivation=step_size_preactivation, forgetting_preactivation=forgetting_preactivation, extra_forgetting_bias=extra_forgetting_bias, subspace_normalizer_gain=subspace_normalizer_gain, skip_connection_stream=skip_connection_stream, blender_projection_matrix=blender_projection_matrix, specialist_prenormal_gain=specialist_prenormal_gain, cluster_router_chance=cluster_router_chance, specialist_chance_within_cluster=specialist_chance_within_cluster, chosen_specialist_ids=chosen_specialist_ids, specialist_switch_matrix=specialist_switch_matrix, specialist_expansion_matrix=specialist_expansion_matrix, specialist_contraction_matrix=specialist_contraction_matrix)


HIGH = lax.Precision.HIGHEST

def sequence_state_blender(readout_query_vectors, attention_key_vectors, attention_content_vectors, step_size_preactivation, forgetting_preactivation, extra_forgetting_bias, subspace_normalizer_gain):
    token_count = readout_query_vectors.shape[0]
    attention_subspace_count = extra_forgetting_bias.shape[1]

    def divide_among_subspaces(data):
        return data.astype(jnp.float32).reshape(token_count, attention_subspace_count, -1)
    query_rows = divide_among_subspaces(readout_query_vectors)
    key_rows = divide_among_subspaces(attention_key_vectors)
    value_rows = divide_among_subspaces(attention_content_vectors)
    learn_rate = jax.nn.sigmoid(divide_among_subspaces(step_size_preactivation))
    logarithmic_forgetting_amounts = divide_among_subspaces(-jnp.exp(-jax.nn.softplus(-forgetting_preactivation) - 0.5)) + extra_forgetting_bias[:, :, None]
    removal = key_rows / jnp.sqrt(lax.optimization_barrier(jnp.sum(key_rows * key_rows, axis=-1, keepdims=True)) + 1e-06)
    head_dim = key_rows.shape[-1]

    def advance(state_now, inputs):
        query_t, decay_t, key_t, value_t, removal_t, rate_t = inputs
        along_removal = jnp.einsum('hvk,hk->hv', state_now, removal_t, precision=HIGH)
        state_now = state_now * jnp.exp(decay_t)[:, None, :] - along_removal[:, :, None] * (removal_t * rate_t)[:, None, :] + value_t[:, :, None] * key_t[:, None, :]
        return (state_now, jnp.einsum('hvk,hk->hv', state_now, query_t, precision=HIGH))
    initial = jnp.zeros((attention_subspace_count, head_dim, head_dim), jnp.float32)
    _, readout = lax.scan(advance, initial, (query_rows, logarithmic_forgetting_amounts, key_rows, value_rows, removal, learn_rate))
    centered = readout - lax.optimization_barrier(jnp.mean(readout, axis=-1, keepdims=True))
    spread = lax.optimization_barrier(jnp.mean(centered * centered, axis=-1, keepdims=True))
    gains = subspace_normalizer_gain.reshape(attention_subspace_count, head_dim)[None]
    normed = centered * lax.rsqrt(spread + 0.00064) * gains
    return normed.reshape(token_count, attention_subspace_count * head_dim).astype(jnp.bfloat16)

def reference(readout_query_vectors, attention_key_vectors, attention_content_vectors, step_size_preactivation, forgetting_preactivation, extra_forgetting_bias, subspace_normalizer_gain, skip_connection_stream, blender_projection_matrix, specialist_prenormal_gain, cluster_router_chance, specialist_chance_within_cluster, chosen_specialist_ids, specialist_switch_matrix, specialist_expansion_matrix, specialist_contraction_matrix):
    blender_result = sequence_state_blender(readout_query_vectors, attention_key_vectors, attention_content_vectors, step_size_preactivation, forgetting_preactivation, extra_forgetting_bias, subspace_normalizer_gain)
    token_count = blender_result.shape[0]
    group_rows = D // N_TP

    def add_group(running, group):
        first_row = (group * group_rows).astype(jnp.int32)
        columns = lax.dynamic_slice_in_dim(blender_result, first_row, group_rows, 1)
        weight_rows = lax.dynamic_slice_in_dim(blender_projection_matrix, first_row, group_rows, 0)
        term = jnp.dot(columns, weight_rows, preferred_element_type=jnp.float32)
        rounded = lax.optimization_barrier(term.astype(jnp.bfloat16)).astype(jnp.float32)
        return (running + rounded, None)
    branch, _ = lax.scan(add_group, jnp.zeros((token_count, D), jnp.float32), jnp.arange(N_TP, dtype=jnp.int32))
    hidden_state = skip_connection_stream.astype(jnp.float32) + branch
    inverse_rms = lax.rsqrt(lax.optimization_barrier(jnp.mean(hidden_state * hidden_state, axis=1, keepdims=True)) + 1e-06)
    normed = (hidden_state * inverse_rms * specialist_prenormal_gain).astype(jnp.bfloat16)
    flat_expert = chosen_specialist_ids.reshape(N_SP, TOK_DEV * TOP)
    one_hot = (flat_expert[:, :, None] == jnp.arange(EXPERTS, dtype=jnp.int32)[None, None, :]).astype(jnp.int32)
    earlier = lax.optimization_barrier(jnp.sum((jnp.cumsum(one_hot, axis=1) - one_hot) * one_hot, axis=2))
    source = jnp.arange(N_SP, dtype=jnp.int32)[:, None]
    slot_index = (flat_expert * (N_SP * CAP) + source * CAP + earlier).reshape(-1)
    token_of = jnp.arange(N_SP * TOK_DEV * TOP, dtype=jnp.int32) // TOP
    slot_owner = jnp.full((EXPERTS * N_SP * CAP,), N_SP * TOK_DEV, jnp.int32).at[slot_index].set(token_of)
    padded = jnp.concatenate([normed, jnp.zeros((1, D), jnp.bfloat16)], axis=0)

    def expert_rows(operands):
        owners, w_gate, w_up, w_down = operands
        rows_in = padded[owners]
        gate_act = jnp.dot(rows_in, w_gate, preferred_element_type=jnp.float32)
        upward = jnp.dot(rows_in, w_up, preferred_element_type=jnp.float32)
        hidden = (jax.nn.silu(gate_act) * upward).astype(jnp.bfloat16)
        unit_group = w_down.shape[0] // N_TP
        hidden_split = hidden.astype(jnp.float32).reshape(-1, N_TP, unit_group)
        down_split = w_down.astype(jnp.float32).reshape(N_TP, unit_group, D)
        partial_value = jnp.einsum('rtf,tfd->trd', hidden_split, down_split)
        rounded = lax.optimization_barrier(partial_value.astype(jnp.bfloat16)).astype(jnp.float32)
        return lax.optimization_barrier(jnp.sum(rounded, axis=0))
    results = lax.map(expert_rows, (slot_owner.reshape(EXPERTS, N_SP * CAP), specialist_switch_matrix, specialist_expansion_matrix, specialist_contraction_matrix))
    picked = results.reshape(-1, D)[slot_index].reshape(N_SP * TOK_DEV, TOP, D)
    route_weight = cluster_router_chance[:, None] * specialist_chance_within_cluster / lax.optimization_barrier(jnp.sum(specialist_chance_within_cluster, axis=1, keepdims=True))
    mixture = lax.optimization_barrier(jnp.sum(route_weight[:, :, None] * picked, axis=1))
    return (hidden_state + mixture).astype(jnp.bfloat16)
```

```python
import functools
import math

import jax
import jax.numpy as jnp
from jax import lax
from jax.experimental import pallas as pl
from jax.experimental.pallas import tpu as pltpu
from jax.sharding import PartitionSpec as P

MESH = pl.DeviceIdType.MESH
F32 = jnp.float32
BF16 = jnp.bfloat16


def dot(left, right, axes=(1, 0)):
    return lax.dot_general(
        left, right, (((axes[0],), (axes[1],)), ((), ())), preferred_element_type=F32
    )


def halves(data):
    high = data.astype(BF16)
    return high, (data - high.astype(F32)).astype(BF16)


def stack(*parts):
    return jnp.concatenate(parts, axis=0)


def beside(*parts):
    return jnp.concatenate(parts, axis=1)


def mixer_setup(head_dim, segment, pairs):
    width = 2 * head_dim
    row = lax.broadcasted_iota(jnp.int32, (segment, width), 0)
    lane = lax.broadcasted_iota(jnp.int32, (segment, width), 1)
    col = lane & (segment - 1)
    return row, lane, col


def split_pair(head_dim):
    def pick(data):
        lane = lax.broadcasted_iota(jnp.int32, data.shape, 1)
        zero = jnp.zeros_like(data)
        return stack(jnp.where(lane < head_dim, data, zero), jnp.where(lane < head_dim, zero, data))

    return pick


def thirds(data):
    high = data.astype(BF16)
    rest = data - high.astype(F32)
    middle = rest.astype(BF16)
    return high, middle, (rest - middle.astype(F32)).astype(BF16)


def mixer_body(head_dim, segment, q_ref, k_ref, v_ref, a_ref, f_ref, b_ref, emit_map, emit_rows):
    rows, channels = q_ref.shape
    width = 2 * head_dim
    pairs = channels // width
    heads = channels // head_dim
    blocks = rows // segment
    shift = segment.bit_length() - 1
    row, lane, col = mixer_setup(head_dim, segment, pairs)
    strict, inclusive = row > col, row >= col
    bd = split_pair(head_dim)
    own = lax.broadcasted_iota(jnp.int32, (width, width), 0) // head_dim == (
        lax.broadcasted_iota(jnp.int32, (width, width), 1) // head_dim
    )
    ones = jnp.where(own, 1.0, 0.0).astype(BF16)
    ones = stack(ones, ones)
    spread = jnp.where(
        lax.rem(lax.broadcasted_iota(jnp.int32, (3 * heads, channels), 0), heads)
        == lax.broadcasted_iota(jnp.int32, (3 * heads, channels), 1) // head_dim,
        1.0,
        0.0,
    ).astype(BF16)
    pieces = stack(*[piece.astype(F32) for piece in thirds(b_ref[...])]).astype(BF16)
    bias = dot(pieces, spread, (0, 0))
    t0 = lax.broadcasted_iota(jnp.int32, (segment, segment), 0)
    t1 = lax.broadcasted_iota(jnp.int32, (segment, segment), 1)
    triangle = jnp.where(t0 >= t1, 1.0, 0.0).astype(BF16)
    triangle = beside(triangle, triangle, triangle)
    chains = [(p, b) for p in range(pairs) for b in range(blocks)]

    def prepare(p, b):
        at = (slice(b * segment, (b + 1) * segment), slice(p * width, (p + 1) * width))
        decay = -(0.6065306597126334 / (1.0 + jnp.exp(-f_ref[at]))) + bias[at]
        cumulative = dot(triangle, stack(*thirds(decay)))
        keys = k_ref[at].astype(F32)
        norms = dot(beside(*halves(keys * keys)), ones)
        removal = keys * lax.rsqrt(norms + 1e-06)
        beta = removal * (1.0 / (1.0 + jnp.exp(-a_ref[at].astype(F32))))
        closing = cumulative[segment - 1 :, :]
        grow = jnp.exp(-cumulative)
        fade = jnp.exp(closing - cumulative)
        c = {}
        c["alpha"] = -removal * jnp.exp(cumulative - decay)
        c["query"] = q_ref[at].astype(F32) * jnp.exp(cumulative)
        c["beta_hat"] = beta * grow
        c["key_hat"] = (keys * grow).astype(BF16)
        c["beta_bar"] = beta * fade
        c["key_bar"] = (keys * fade).astype(BF16)
        c["keep"] = jnp.where(row == col, jnp.exp(closing), 0.0)
        c["values"] = v_ref[at]
        return c

    C = [prepare(p, b) for p, b in chains]

    for c in C:
        ah, al = halves(c["alpha"])
        bh, bl = halves(c["beta_hat"])
        qh = c["query"].astype(BF16)
        by_beta = dot(stack(ah, al, qh), bd(bh), (1, 1))
        low = dot(ah, bd(bl), (1, 1))
        by_key = dot(stack(ah, qh), bd(c["key_hat"]), (1, 1))
        c["lower"] = jnp.where(strict, by_beta[:segment] + by_beta[segment : 2 * segment] + low, 0.0)
        c["read_remove"] = jnp.where(inclusive, by_beta[2 * segment :], 0.0).astype(BF16)
        c["remove_write"] = jnp.where(strict, by_key[:segment], 0.0)
        c["read_write"] = jnp.where(inclusive, by_key[segment:], 0.0).astype(BF16)
        c["ah"] = ah
        c["lh"], c["ll"] = halves(c["lower"])
    for c in C:
        wh, wl = halves(c["remove_write"])
        product = dot(stack(wh, wl, c["read_write"]), bd(c["values"]))
        c["side"] = product[:segment] + product[segment : 2 * segment]
        c["local"] = product[2 * segment :]
        c["inverse"] = jnp.where(
            row == col, 1.0, jnp.where((row >> 1) == (col >> 1), c["lower"], 0.0)
        )
    zero = jnp.zeros((segment, width), BF16)
    for s in range(1, shift):
        off = ((row >> (s + 1)) == (col >> (s + 1))) & ((row >> s) != (col >> s))
        for c in C:
            c["near"] = c["inverse"].astype(BF16)
            c["reach"] = dot(jnp.where(off, c["lh"], zero), bd(c["near"]))
        for c in C:
            c["inverse"] = c["inverse"] + dot(c["near"], bd(c["reach"].astype(BF16)))
    for c in C:
        c["near"] = c["inverse"].astype(BF16)
        c["both"] = beside(c["alpha"], c["side"])
        c["solved"] = dot(c["near"], beside(bd(c["ah"]), bd(c["side"].astype(BF16))))
    for c in C:
        sh, sl = halves(c["solved"])
        high = dot(stack(c["lh"], c["ll"]), beside(bd(sh[:, :width]), bd(sh[:, width:])))
        low = dot(c["lh"], beside(bd(sl[:, :width]), bd(sl[:, width:])))
        c["miss"] = c["both"] - c["solved"] + (high[:segment] + (high[segment:] + low))
    for c in C:
        miss = c["miss"].astype(BF16)
        c["solved"] = c["solved"] + dot(c["near"], beside(bd(miss[:, :width]), bd(miss[:, width:])))
    for c in C:
        sh, sl = halves(c["solved"])
        c["sh"] = sh
        bh, bl = halves(c["beta_bar"])
        left = stack(sh, sl, sh, beside(zero, c["values"]))
        step = dot(left, stack(bh, bh, bl, c["key_bar"]), (0, 0))
        first = lane < head_dim
        c["keep"] = c["keep"] + jnp.where(first, step[:head_dim], step[head_dim:width])
        c["add"] = jnp.where(first, step[width : width + head_dim], step[width + head_dim :])
    states = [[None] for _ in range(pairs)]
    now = [stack(C[p * blocks]["keep"], C[p * blocks]["add"]) for p in range(pairs)]
    for b in range(1, blocks):
        for p in range(pairs):
            c = C[p * blocks + b]
            kh, kl = halves(c["keep"])
            th, tl = halves(now[p])
            states[p].append(th)
            high = dot(stack(th, tl), bd(kh))
            low = dot(th, bd(kl))
            total = high[:width] + (high[width:] + low)
            now[p] = stack(total[:head_dim], total[head_dim:] + c["add"])
    for p in range(pairs):
        emit_map(p, now[p])
    for i, (p, b) in enumerate(chains):
        c = C[i]
        sh = c["sh"]
        read = dot(c["read_remove"], beside(bd(sh[:, :width]), bd(sh[:, width:])))
        c["read_map"] = c["query"] + read[:, :width]
        c["local"] = c["local"] + read[:, width:]
    for i, (p, b) in enumerate(chains):
        c = C[i]
        maps, local = c["read_map"].astype(BF16), c["local"]
        if b:
            th = states[p][b]
            seen = dot(maps, stack(bd(th[:head_dim]), bd(th[head_dim:])), (1, 1))
            maps, local = seen[:, :width].astype(BF16), local + seen[:, width:]
        emit_rows(p, b, maps, local)


def mixer_kernel(head_dim, segment, q_ref, k_ref, v_ref, a_ref, f_ref, b_ref, out_ref, map_ref, ka_ref):
    width = 2 * head_dim

    def emit_map(p, state):
        for h in range(2):
            part = slice(h * head_dim, (h + 1) * head_dim)
            both = beside(state[:head_dim, part], state[head_dim:, part])
            ka_ref[2 * p + h] = both.astype(BF16)

    def emit_rows(p, b, maps, local):
        at = (slice(b * segment, (b + 1) * segment), slice(p * width, (p + 1) * width))
        out_ref[at] = local
        map_ref[at] = maps

    mixer_body(head_dim, segment, q_ref, k_ref, v_ref, a_ref, f_ref, b_ref, emit_map, emit_rows)


def exchange_kernel(count, per, workers, ka_ref, st_ref, got, fold, send1, recv1, send2, recv2):
    me = lax.axis_index("sp")
    dim = ka_ref.shape[1]
    barrier = pltpu.get_barrier_semaphore()
    for d in range(1, count):
        pl.semaphore_signal(
            barrier, inc=1, device_id={"sp": lax.rem(me + d, count)}, device_id_type=MESH
        )
    pl.semaphore_wait(barrier, count - 1)

    def first(t, owner):
        return pltpu.make_async_remote_copy(
            src_ref=ka_ref.at[pl.ds(t * per, per)],
            dst_ref=got.at[owner],
            send_sem=send1.at[t],
            recv_sem=recv1.at[owner],
            device_id={"sp": t},
            device_id_type=MESH,
        )

    def second(t, owner):
        return pltpu.make_async_remote_copy(
            src_ref=fold.at[t],
            dst_ref=st_ref.at[pl.ds(owner * per, per)],
            send_sem=send2.at[t],
            recv_sem=recv2.at[owner],
            device_id={"sp": t},
            device_id_type=MESH,
        )

    for t in range(workers):
        @pl.when(t != me)
        def _(t=t):
            first(t, me).start()

    def work():
        got[me] = ka_ref[pl.ds(me * per, per)]
        state = [jnp.zeros((dim, dim), F32) for _ in range(per)]
        for j in range(count):
            @pl.when(j != me)
            def _(j=j):
                pltpu.make_async_remote_copy(
                    src_ref=got.at[j],
                    dst_ref=got.at[j],
                    send_sem=send1.at[0],
                    recv_sem=recv1.at[j],
                    device_id={"sp": j},
                    device_id_type=MESH,
                ).wait_recv()
            for i in range(per):
                fold[j, i] = jnp.concatenate([state[i], jnp.zeros_like(state[i])], axis=1).astype(BF16)
                both = got[j, i]
                keep, add = both[:, :dim], both[:, dim:].astype(F32)
                sh, sl = halves(state[i])
                state[i] = dot(sh, keep) + dot(sl, keep) + add
        for t in range(count):
            @pl.when(t != me)
            def _(t=t):
                second(t, me).start()
        st_ref[pl.ds(me * per, per)] = fold[me]
        for t in range(count):
            @pl.when(t != me)
            def _(t=t):
                second(t, me).wait_send()

    if workers == count:
        work()
    else:
        pl.when(me < workers)(work)
    for t in range(workers):
        @pl.when(t != me)
        def _(t=t):
            first(t, me).wait_send()
            pltpu.make_async_remote_copy(
                src_ref=fold.at[t],
                dst_ref=st_ref.at[pl.ds(t * per, per)],
                send_sem=send2.at[0],
                recv_sem=recv2.at[t],
                device_id={"sp": t},
                device_id_type=MESH,
            ).wait_recv()


def finish_kernel(head_dim, out_ref, map_ref, st_ref, gain_ref, w_ref, part_ref, mixed):
    @pl.when(pl.program_id(0) == 0)
    def _():
        for h in range(out_ref.shape[1] // head_dim):
            part = slice(h * head_dim, (h + 1) * head_dim)
            states = st_ref[h][:, :head_dim]
            output = out_ref[:, part] + dot(map_ref[:, part], states, (1, 1))
            centered = output - jnp.mean(output, axis=1, keepdims=True)
            spread = jnp.mean(centered * centered, axis=1, keepdims=True)
            mixed[:, part] = (centered * lax.rsqrt(spread + 0.00064) * gain_ref[:, part]).astype(BF16)

    part_ref[...] = dot(mixed[...], w_ref[...]).astype(BF16)


def mixer_branch(query, key, value, step, forget, bias, gain, blender):
    count = lax.axis_size("sp")
    rows, channels = query.shape
    heads = bias.shape[1]
    head_dim = channels // heads
    segment = min(64, rows)
    width = 2 * head_dim
    vmem = pl.BlockSpec(memory_space=pltpu.VMEM)
    out, maps, ka = pl.pallas_call(
        functools.partial(mixer_kernel, head_dim, segment),
        in_specs=[vmem] * 6,
        out_specs=[vmem] * 3,
        out_shape=[
            jax.ShapeDtypeStruct((rows, channels), F32),
            jax.ShapeDtypeStruct((rows, channels), BF16),
            jax.ShapeDtypeStruct((heads, head_dim, width), BF16),
        ],
        compiler_params=pltpu.CompilerParams(vmem_limit_bytes=56 * 1024 * 1024),
    )(query, key, value, step, forget, bias.T)
    per = max(1, heads // count)
    workers = heads // per
    states = pl.pallas_call(
        functools.partial(exchange_kernel, count, per, workers),
        out_shape=jax.ShapeDtypeStruct((heads, head_dim, width), BF16),
        in_specs=[vmem],
        out_specs=vmem,
        scratch_shapes=[
            pltpu.VMEM((count, per, head_dim, width), BF16),
            pltpu.VMEM((count, per, head_dim, width), BF16),
            pltpu.SemaphoreType.DMA((count,)),
            pltpu.SemaphoreType.DMA((count,)),
            pltpu.SemaphoreType.DMA((count,)),
            pltpu.SemaphoreType.DMA((count,)),
        ],
        compiler_params=pltpu.CompilerParams(collective_id=1, has_side_effects=True),
    )(ka)
    model_width = blender.shape[1]
    tile = min(512, model_width)
    whole = lambda *shape: pl.BlockSpec(shape, lambda p: (0,) * len(shape))
    return pl.pallas_call(
        functools.partial(finish_kernel, head_dim),
        grid=(model_width // tile,),
        in_specs=[
            whole(rows, channels),
            whole(rows, channels),
            whole(heads, head_dim, width),
            whole(1, channels),
            pl.BlockSpec((channels, tile), lambda p: (0, p)),
        ],
        out_specs=pl.BlockSpec((rows, tile), lambda p: (0, p)),
        out_shape=jax.ShapeDtypeStruct((rows, model_width), BF16),
        scratch_shapes=[pltpu.VMEM((rows, channels), BF16)],
    )(out, maps, states, gain.reshape(1, channels), blender)


def greet(sp_count, tp_count, sp, tp):
    barrier = pltpu.get_barrier_semaphore()
    for d in range(1, sp_count):
        pl.semaphore_signal(
            barrier, inc=1, device_id={"sp": lax.rem(sp + d, sp_count)}, device_id_type=MESH
        )
    for d in range(1, tp_count):
        pl.semaphore_signal(
            barrier, inc=1, device_id={"tp": lax.rem(tp + d, tp_count)}, device_id_type=MESH
        )
    pl.semaphore_wait(barrier, sp_count + tp_count - 2)


def copy_to(src, dst, send, recv, device):
    return pltpu.make_async_remote_copy(
        src_ref=src,
        dst_ref=dst,
        send_sem=send,
        recv_sem=recv,
        device_id=device,
        device_id_type=MESH,
    )


def span(index, size):
    return pl.ds(pl.multiple_of(index * size, size), size)


def row_total(data, terms):
    ones = jnp.ones((8, data.shape[1]), BF16)
    total = None
    for _ in range(terms):
        piece = data.astype(BF16)
        data = data - piece.astype(F32)
        product = dot(ones, piece, (1, 1))
        total = product if total is None else total + product
    return total


def route_kernel(
    sp_count, tp_count, experts, capacity,
    part_ref, skip_ref, gain_ref, ids_ref,
    hidden_ref, slot_ref, rows_ref,
    gathered, squares, outgoing,
    s_part, r_part, s_sq, r_sq, s_out, r_out, s_own, s_fwd, r_col,
):
    sp, tp = lax.axis_index("sp"), lax.axis_index("tp")
    rows, model = part_ref.shape
    cols = model // tp_count
    mine = span(tp, cols)
    groups = tp_count // 2
    core, group = lax.rem(tp, 2), tp // 2
    sibling = group * 2 + 1 - core
    greet(sp_count, tp_count, sp, tp)

    def part_copy(p):
        return copy_to(
            part_ref.at[:, span(p, cols)], gathered.at[tp], s_part.at[p], r_part.at[tp], {"tp": p}
        )

    for d in range(1, tp_count):
        part_copy(lax.rem(tp + d, tp_count)).start()

    ids = ids_ref[...]
    top = ids.shape[1]
    lanes = lax.broadcasted_iota(jnp.int32, (rows, experts), 1)
    named = [ids[:, k : k + 1] == lanes for k in range(top)]
    anyone = sum(jnp.where(n, 1.0, 0.0) for n in named).astype(BF16)
    r0 = lax.broadcasted_iota(jnp.int32, (rows, rows), 0)
    r1 = lax.broadcasted_iota(jnp.int32, (rows, rows), 1)
    before = dot(jnp.where(r0 > r1, 1.0, 0.0).astype(BF16), anyone)
    slots = [
        jnp.sum(
            jnp.where(n, before + lanes.astype(F32) * capacity, 0.0), axis=1, keepdims=True
        ).astype(jnp.int32)
        for n in named
    ]
    slot_ref[...] = jnp.concatenate(slots, axis=1)

    branch = part_ref[:, mine].astype(F32)
    for d in range(1, tp_count):
        p = lax.rem(tp + d, tp_count)
        copy_to(gathered.at[p], gathered.at[p], s_part.at[p], r_part.at[p], {"tp": p}).wait_recv()
        branch = branch + gathered[p].astype(F32)
    hidden = skip_ref[:, mine].astype(F32) + branch
    hidden_ref[...] = hidden
    squares[tp] = row_total(hidden * hidden, 3)

    def square_copy(p):
        return copy_to(squares.at[tp], squares.at[tp], s_sq.at[p], r_sq.at[tp], {"tp": p})

    for d in range(1, tp_count):
        square_copy(lax.rem(tp + d, tp_count)).start()
    total = squares[tp]
    for d in range(1, tp_count):
        p = lax.rem(tp + d, tp_count)
        copy_to(squares.at[p], squares.at[p], s_sq.at[p], r_sq.at[p], {"tp": p}).wait_recv()
        total = total + squares[p]
    inverse = lax.rsqrt(total / model + 1e-06)
    first = jnp.where(lax.broadcasted_iota(jnp.int32, (8, 128), 0) == 0, 1.0, 0.0).astype(BF16)
    column = None
    for _ in range(3):
        piece = inverse.astype(BF16)
        inverse = inverse - piece.astype(F32)
        product = dot(piece, first, (0, 0))
        column = product if column is None else column + product
    normed = (hidden * column[:, :1] * gain_ref[:, mine]).astype(BF16)

    per = experts // sp_count * capacity
    places = lax.broadcasted_iota(jnp.int32, (rows, per), 1)

    def block_for(t):
        at = places + t * per
        chosen = (slots[0] == at)
        for s in slots[1:]:
            chosen = chosen | (s == at)
        return dot(jnp.where(chosen, 1.0, 0.0).astype(BF16), normed, (0, 0)).astype(BF16)

    def out_copy(t):
        return copy_to(
            outgoing.at[t], rows_ref.at[sp, :, mine], s_out.at[t], r_out.at[sp], {"sp": t}
        )

    def give(d, carry):
        t = lax.rem(sp + d, sp_count)
        outgoing[t] = block_for(t)
        out_copy(t).start()
        return carry

    lax.fori_loop(1, sp_count, give, 0)
    rows_ref[sp, :, mine] = block_for(sp)

    def own_copy(p, s):
        here = rows_ref.at[s, :, mine]
        return copy_to(here, here, s_own.at[p, s], r_col.at[tp, s], {"tp": p})

    def forward(o, s):
        here = rows_ref.at[s, :, span(o, cols)]
        return copy_to(here, here, s_fwd.at[o, s], r_col.at[o, s], {"tp": sibling})

    def arrived(o, s):
        here = rows_ref.at[s, :, span(o, cols)]
        copy_to(here, here, s_fwd.at[o, s], r_col.at[o, s], {"tp": sibling}).wait_recv()

    def peers():
        return [lax.rem(group + g, groups) * 2 + core for g in range(1, groups)]

    lag = 2

    def relay(d, carry):
        @pl.when(d < sp_count)
        def _():
            s = lax.rem(sp - d + sp_count, sp_count)

            @pl.when(d > 0)
            def _():
                here = rows_ref.at[s, :, mine]
                copy_to(here, here, s_out.at[s], r_out.at[s], {"sp": s}).wait_recv()

            for p in peers():
                own_copy(p, s).start()
            own_copy(sibling, s).start()

        @pl.when(d >= lag)
        def _():
            s = lax.rem(sp - (d - lag) + sp_count, sp_count)
            for o in peers():
                arrived(o, s)
                forward(o, s).start()

        return carry

    lax.fori_loop(0, sp_count + lag, relay, 0)

    def settle(s, carry):
        arrived(sibling, s)
        for g in range(1, groups):
            arrived(lax.rem(group + g, groups) * 2 + 1 - core, s)
        own_copy(sibling, s).wait_send()
        for p in peers():
            own_copy(p, s).wait_send()
            forward(p, s).wait_send()
        return carry

    lax.fori_loop(0, sp_count, settle, 0)

    def sent(d, carry):
        out_copy(lax.rem(sp + d, sp_count)).wait_send()
        return carry

    lax.fori_loop(1, sp_count, sent, 0)
    for d in range(1, tp_count):
        p = lax.rem(tp + d, tp_count)
        part_copy(p).wait_send()
        square_copy(p).wait_send()


def return_kernel(
    sp_count, tp_count,
    rows_ref, switch_ref, expand_ref, contract_ref, hidden_ref, slot_ref, weight_ref,
    out_ref,
    y_ref, from_sib, pair, from_peer, summed, back,
    s_sib, r_sib, s_peer, r_peer, s_back, r_back, s_own, s_fwd, r_col,
):
    sp, tp = lax.axis_index("sp"), lax.axis_index("tp")
    per, model = y_ref.shape[1:]
    rows = hidden_ref.shape[0]
    cols = model // tp_count
    mine = span(tp, cols)
    groups = tp_count // 2
    core, group = lax.rem(tp, 2), tp // 2
    sibling = group * 2 + 1 - core
    greet(sp_count, tp_count, sp, tp)

    def sib_copy(s, g):
        return copy_to(
            y_ref.at[s, :, span(g * 2 + 1 - core, cols)],
            from_sib.at[s, g],
            s_sib.at[s, g],
            r_sib.at[s, g],
            {"tp": sibling},
        )

    def peer_copy(s, g):
        return copy_to(
            pair.at[s, g],
            from_peer.at[s, group],
            s_peer.at[s, g],
            r_peer.at[s, group],
            {"tp": g * 2 + core},
        )

    def back_copy(t):
        return copy_to(summed.at[t], back.at[sp], s_back.at[t], r_back.at[sp], {"sp": t})

    def others():
        return [lax.rem(group + d, groups) for d in range(1, groups)]

    def order(d):
        return lax.rem(sp + 1 + d, sp_count)

    local = switch_ref.shape[0]
    capacity = per // local
    chunk = math.gcd(sp_count, max(1, 256 // capacity))
    chunks = sp_count // chunk

    def expert(i):
        at = [order(i * chunk + c) for c in range(chunk)]
        for e in range(local):
            inside = slice(e * capacity, (e + 1) * capacity)
            data = jnp.concatenate([rows_ref[s, inside, :] for s in at], axis=0)
            gate = dot(data, switch_ref[e])
            units = (gate / (1.0 + jnp.exp(-gate)) * dot(data, expand_ref[e])).astype(BF16)
            value = dot(units, contract_ref[e]).astype(BF16)
            for c in range(chunk):
                y_ref[at[c], inside, :] = value[c * capacity : (c + 1) * capacity]
        for s in at:
            for g in others():
                sib_copy(s, g).start()
            sib_copy(s, group).start()

    def meet(s):
        for g in others():
            sib_copy(s, g).wait_recv()
            pair[s, g] = (
                y_ref[s, :, span(g * 2 + core, cols)].astype(F32) + from_sib[s, g].astype(F32)
            ).astype(BF16)
            peer_copy(s, g).start()
        sib_copy(s, group).wait_recv()

    def total_up(s):
        total = y_ref[s, :, mine].astype(F32) + from_sib[s, group].astype(F32)
        for g in others():
            copy_to(
                from_peer.at[s, g],
                from_peer.at[s, g],
                s_peer.at[s, g],
                r_peer.at[s, g],
                {"tp": g * 2 + core},
            ).wait_recv()
            total = total + from_peer[s, g].astype(F32)

        @pl.when(s != sp)
        def _():
            summed[s] = total.astype(BF16)
            back_copy(s).start()

        @pl.when(s == sp)
        def _():
            back[s] = total.astype(BF16)

    def step(i, carry):
        @pl.when(i < chunks)
        def _():
            expert(i)

        @pl.when((i >= 1) & (i <= chunks))
        def _():
            for c in range(chunk):
                meet(order((i - 1) * chunk + c))

        @pl.when(i >= 2)
        def _():
            for c in range(chunk):
                total_up(order((i - 2) * chunk + c))

        return carry

    lax.fori_loop(0, chunks + 2, step, 0)
    slots = slot_ref[...]
    weights = weight_ref[...]
    places = lax.broadcasted_iota(jnp.int32, (rows, sp_count * per), 1)
    top = slots.shape[1]
    chosen = [jnp.where(slots[:, k : k + 1] == places, 1.0, 0.0).astype(BF16) for k in range(top)]

    def landed(d, carry):
        s = lax.rem(sp + d, sp_count)
        copy_to(back.at[s], back.at[s], s_back.at[s], r_back.at[s], {"sp": s}).wait_recv()
        return carry

    lax.fori_loop(1, sp_count, landed, 0)
    returned = back[...].reshape(sp_count * per, cols)
    result = hidden_ref[...] + sum(
        weights[:, k : k + 1] * dot(chosen[k], returned) for k in range(top)
    )
    out_ref[:, mine] = result.astype(BF16)

    def own_copy(p):
        here = out_ref.at[:, mine]
        return copy_to(here, here, s_own.at[p], r_col.at[tp], {"tp": p})

    def forward(o):
        here = out_ref.at[:, span(o, cols)]
        return copy_to(here, here, s_fwd.at[o], r_col.at[o], {"tp": sibling})

    peers = [g * 2 + core for g in others()]
    for p in peers:
        own_copy(p).start()
    own_copy(sibling).start()
    for p in peers:
        forward(p).wait_recv()
        forward(p).start()
    forward(sibling).wait_recv()
    for g in others():
        forward(g * 2 + 1 - core).wait_recv()
    own_copy(sibling).wait_send()
    for p in peers:
        own_copy(p).wait_send()
        forward(p).wait_send()

    def close(s, carry):
        sib_copy(s, group).wait_send()
        for g in others():
            sib_copy(s, g).wait_send()
            peer_copy(s, g).wait_send()
        return carry

    lax.fori_loop(0, sp_count, close, 0)

    def sent(d, carry):
        back_copy(lax.rem(sp + d, sp_count)).wait_send()
        return carry

    lax.fori_loop(1, sp_count, sent, 0)


def body(
    readout_query_vectors,
    attention_key_vectors,
    attention_content_vectors,
    step_size_preactivation,
    forgetting_preactivation,
    extra_forgetting_bias,
    subspace_normalizer_gain,
    skip_connection_stream,
    blender_projection_matrix,
    specialist_prenormal_gain,
    cluster_router_chance,
    specialist_chance_within_cluster,
    chosen_specialist_ids,
    specialist_switch_matrix,
    specialist_expansion_matrix,
    specialist_contraction_matrix,
):
    partial_branch = mixer_branch(
        readout_query_vectors,
        attention_key_vectors,
        attention_content_vectors,
        step_size_preactivation,
        forgetting_preactivation,
        extra_forgetting_bias,
        subspace_normalizer_gain,
        blender_projection_matrix,
    )
    tok_rows, model_width = skip_connection_stream.shape
    sp_count, tp_count = lax.axis_size("sp"), lax.axis_size("tp")
    local_experts = specialist_switch_matrix.shape[0]
    experts = local_experts * sp_count
    top_count = chosen_specialist_ids.shape[1]
    capacity = 2 * tok_rows * top_count // experts
    cols = model_width // tp_count
    per = local_experts * capacity
    groups = tp_count // 2
    vmem = pl.BlockSpec(memory_space=pltpu.VMEM)
    sems = pltpu.SemaphoreType.DMA
    hidden_cols, slots, rows_in = pl.pallas_call(
        functools.partial(route_kernel, sp_count, tp_count, experts, capacity),
        out_shape=[
            jax.ShapeDtypeStruct((tok_rows, cols), F32),
            jax.ShapeDtypeStruct((tok_rows, top_count), jnp.int32),
            jax.ShapeDtypeStruct((sp_count, per, model_width), BF16),
        ],
        in_specs=[vmem] * 4,
        out_specs=[vmem] * 3,
        scratch_shapes=[
            pltpu.VMEM((tp_count, tok_rows, cols), BF16),
            pltpu.VMEM((tp_count, 8, tok_rows), F32),
            pltpu.VMEM((sp_count, per, cols), BF16),
            sems((tp_count,)),
            sems((tp_count,)),
            sems((tp_count,)),
            sems((tp_count,)),
            sems((sp_count,)),
            sems((sp_count,)),
            sems((tp_count, sp_count)),
            sems((tp_count, sp_count)),
            sems((tp_count, sp_count)),
        ],
        compiler_params=pltpu.CompilerParams(
            collective_id=2, has_side_effects=True, vmem_limit_bytes=40 * 1024 * 1024
        ),
    )(
        partial_branch,
        skip_connection_stream,
        specialist_prenormal_gain.reshape(1, model_width),
        chosen_specialist_ids,
    )
    route_weight = (
        cluster_router_chance[:, None]
        * specialist_chance_within_cluster
        / jnp.sum(specialist_chance_within_cluster, axis=1, keepdims=True)
    )
    return pl.pallas_call(
        functools.partial(return_kernel, sp_count, tp_count),
        out_shape=jax.ShapeDtypeStruct((tok_rows, model_width), BF16),
        in_specs=[vmem] * 7,
        out_specs=vmem,
        scratch_shapes=[
            pltpu.VMEM((sp_count, per, model_width), BF16),
            pltpu.VMEM((sp_count, groups, per, cols), BF16),
            pltpu.VMEM((sp_count, groups, per, cols), BF16),
            pltpu.VMEM((sp_count, groups, per, cols), BF16),
            pltpu.VMEM((sp_count, per, cols), BF16),
            pltpu.VMEM((sp_count, per, cols), BF16),
            sems((sp_count, groups)),
            sems((sp_count, groups)),
            sems((sp_count, groups)),
            sems((sp_count, groups)),
            sems((sp_count,)),
            sems((sp_count,)),
            sems((tp_count,)),
            sems((tp_count,)),
            sems((tp_count,)),
        ],
        compiler_params=pltpu.CompilerParams(
            collective_id=3, has_side_effects=True, vmem_limit_bytes=50 * 1024 * 1024
        ),
    )(
        rows_in,
        specialist_switch_matrix,
        specialist_expansion_matrix,
        specialist_contraction_matrix,
        hidden_cols,
        slots,
        route_weight,
    )


def solution(mesh):
    in_specs = (
        P("sp", "tp"),
        P("sp", "tp"),
        P("sp", "tp"),
        P("sp", "tp"),
        P("sp", "tp"),
        P("sp", "tp"),
        P("tp"),
        P("sp", None),
        P("tp", None),
        P(),
        P("sp"),
        P("sp", None),
        P("sp", None),
        P("sp", None, "tp"),
        P("sp", None, "tp"),
        P("sp", "tp", None),
    )
    out_specs = P("sp", None)
    return jax.shard_map(body, mesh=mesh, in_specs=in_specs, out_specs=out_specs, check_vma=False)
```

```python
import functools
import math

import jax
import jax.numpy as jnp
from jax import lax
from jax.experimental import pallas as pl
from jax.experimental.pallas import tpu as pltpu
from jax.sharding import PartitionSpec as P

MESH = pl.DeviceIdType.MESH
F32 = jnp.float32
BF16 = jnp.bfloat16
VMEM_LIMIT = 63 * 1024 * 1024


def dot(left, right, axes=(1, 0)):
    return lax.dot_general(
        left, right, (((axes[0],), (axes[1],)), ((), ())), preferred_element_type=F32
    )


def halves(data):
    high = data.astype(BF16)
    return high, (data - high.astype(F32)).astype(BF16)


def stack(*parts):
    return jnp.concatenate(parts, axis=0)


def beside(*parts):
    return jnp.concatenate(parts, axis=1)


def mixer_setup(head_dim, segment, pairs):
    width = 2 * head_dim
    row = lax.broadcasted_iota(jnp.int32, (segment, width), 0)
    lane = lax.broadcasted_iota(jnp.int32, (segment, width), 1)
    col = lane & (segment - 1)
    return row, lane, col


def split_pair(head_dim):
    def pick(data):
        lane = lax.broadcasted_iota(jnp.int32, data.shape, 1)
        zero = jnp.zeros_like(data)
        return stack(jnp.where(lane < head_dim, data, zero), jnp.where(lane < head_dim, zero, data))

    return pick


def thirds(data):
    high = data.astype(BF16)
    rest = data - high.astype(F32)
    middle = rest.astype(BF16)
    return high, middle, (rest - middle.astype(F32)).astype(BF16)


def mixer_body(head_dim, segment, q_ref, k_ref, v_ref, a_ref, f_ref, b_ref, emit_map, between, emit_rows):
    rows, channels = q_ref.shape
    width = 2 * head_dim
    pairs = channels // width
    heads = channels // head_dim
    blocks = rows // segment
    shift = segment.bit_length() - 1
    row, lane, col = mixer_setup(head_dim, segment, pairs)
    strict, inclusive = row > col, row >= col
    bd = split_pair(head_dim)
    own = lax.broadcasted_iota(jnp.int32, (width, width), 0) // head_dim == (
        lax.broadcasted_iota(jnp.int32, (width, width), 1) // head_dim
    )
    ones = jnp.where(own, 1.0, 0.0).astype(BF16)
    ones = stack(ones, ones)
    spread = jnp.where(
        lax.rem(lax.broadcasted_iota(jnp.int32, (3 * heads, channels), 0), heads)
        == lax.broadcasted_iota(jnp.int32, (3 * heads, channels), 1) // head_dim,
        1.0,
        0.0,
    ).astype(BF16)
    pieces = stack(*[piece.astype(F32) for piece in thirds(b_ref[...])]).astype(BF16)
    bias = dot(pieces, spread, (0, 0))
    t0 = lax.broadcasted_iota(jnp.int32, (segment, segment), 0)
    t1 = lax.broadcasted_iota(jnp.int32, (segment, segment), 1)
    triangle = jnp.where(t0 >= t1, 1.0, 0.0).astype(BF16)
    triangle = beside(triangle, triangle, triangle)
    chains = [(p, b) for p in range(pairs) for b in range(blocks)]

    def prepare(p, b):
        at = (slice(b * segment, (b + 1) * segment), slice(p * width, (p + 1) * width))
        decay = -(0.6065306597126334 / (1.0 + jnp.exp(-f_ref[at]))) + bias[at]
        cumulative = dot(triangle, stack(*thirds(decay)))
        keys = k_ref[at].astype(F32)
        norms = dot(beside(*halves(keys * keys)), ones)
        removal = keys * lax.rsqrt(norms + 1e-06)
        beta = removal * (1.0 / (1.0 + jnp.exp(-a_ref[at].astype(F32))))
        closing = cumulative[segment - 1 :, :]
        grow = jnp.exp(-cumulative)
        fade = jnp.exp(closing - cumulative)
        c = {}
        c["alpha"] = -removal * jnp.exp(cumulative - decay)
        c["query"] = q_ref[at].astype(F32) * jnp.exp(cumulative)
        c["beta_hat"] = beta * grow
        c["key_hat"] = (keys * grow).astype(BF16)
        c["beta_bar"] = beta * fade
        c["key_bar"] = (keys * fade).astype(BF16)
        c["keep"] = jnp.where(row == col, jnp.exp(closing), 0.0)
        c["values"] = v_ref[at]
        return c

    C = [prepare(p, b) for p, b in chains]

    for c in C:
        ah, al = halves(c["alpha"])
        bh, bl = halves(c["beta_hat"])
        qh = c["query"].astype(BF16)
        by_beta = dot(stack(ah, al, qh), bd(bh), (1, 1))
        low = dot(ah, bd(bl), (1, 1))
        by_key = dot(stack(ah, qh), bd(c["key_hat"]), (1, 1))
        c["lower"] = jnp.where(strict, by_beta[:segment] + by_beta[segment : 2 * segment] + low, 0.0)
        c["read_remove"] = jnp.where(inclusive, by_beta[2 * segment :], 0.0).astype(BF16)
        c["remove_write"] = jnp.where(strict, by_key[:segment], 0.0)
        c["read_write"] = jnp.where(inclusive, by_key[segment:], 0.0).astype(BF16)
        c["ah"] = ah
        c["lh"], c["ll"] = halves(c["lower"])
    for c in C:
        wh, wl = halves(c["remove_write"])
        product = dot(stack(wh, wl, c["read_write"]), bd(c["values"]))
        c["side"] = product[:segment] + product[segment : 2 * segment]
        c["local"] = product[2 * segment :]
        c["inverse"] = jnp.where(
            row == col, 1.0, jnp.where((row >> 1) == (col >> 1), c["lower"], 0.0)
        )
    zero = jnp.zeros((segment, width), BF16)
    for s in range(1, shift):
        off = ((row >> (s + 1)) == (col >> (s + 1))) & ((row >> s) != (col >> s))
        for c in C:
            c["near"] = c["inverse"].astype(BF16)
            c["reach"] = dot(jnp.where(off, c["lh"], zero), bd(c["near"]))
        for c in C:
            c["inverse"] = c["inverse"] + dot(c["near"], bd(c["reach"].astype(BF16)))
    for c in C:
        c["near"] = c["inverse"].astype(BF16)
        c["both"] = beside(c["alpha"], c["side"])
        c["solved"] = dot(c["near"], beside(bd(c["ah"]), bd(c["side"].astype(BF16))))
    for c in C:
        sh, sl = halves(c["solved"])
        high = dot(stack(c["lh"], c["ll"]), beside(bd(sh[:, :width]), bd(sh[:, width:])))
        low = dot(c["lh"], beside(bd(sl[:, :width]), bd(sl[:, width:])))
        c["miss"] = c["both"] - c["solved"] + (high[:segment] + (high[segment:] + low))
    for c in C:
        miss = c["miss"].astype(BF16)
        c["solved"] = c["solved"] + dot(c["near"], beside(bd(miss[:, :width]), bd(miss[:, width:])))
    for c in C:
        sh, sl = halves(c["solved"])
        c["sh"] = sh
        bh, bl = halves(c["beta_bar"])
        left = stack(sh, sl, sh, beside(zero, c["values"]))
        step = dot(left, stack(bh, bh, bl, c["key_bar"]), (0, 0))
        first = lane < head_dim
        c["keep"] = c["keep"] + jnp.where(first, step[:head_dim], step[head_dim:width])
        c["add"] = jnp.where(first, step[width : width + head_dim], step[width + head_dim :])
    states = [[None] for _ in range(pairs)]
    now = [stack(C[p * blocks]["keep"], C[p * blocks]["add"]) for p in range(pairs)]
    for b in range(1, blocks):
        for p in range(pairs):
            c = C[p * blocks + b]
            kh, kl = halves(c["keep"])
            th, tl = halves(now[p])
            states[p].append(th)
            high = dot(stack(th, tl), bd(kh))
            low = dot(th, bd(kl))
            total = high[:width] + (high[width:] + low)
            now[p] = stack(total[:head_dim], total[head_dim:] + c["add"])
    for p in range(pairs):
        emit_map(p, now[p])
    between()
    for i, (p, b) in enumerate(chains):
        c = C[i]
        sh = c["sh"]
        read = dot(c["read_remove"], beside(bd(sh[:, :width]), bd(sh[:, width:])))
        c["read_map"] = c["query"] + read[:, :width]
        c["local"] = c["local"] + read[:, width:]
    for i, (p, b) in enumerate(chains):
        c = C[i]
        maps, local = c["read_map"].astype(BF16), c["local"]
        if b:
            th = states[p][b]
            seen = dot(maps, stack(bd(th[:head_dim]), bd(th[head_dim:])), (1, 1))
            maps, local = seen[:, :width].astype(BF16), local + seen[:, width:]
        emit_rows(p, b, maps, local)


def mate(me, d, count):
    total, bit = 0, 1
    while bit < count:
        own = lax.rem(lax.div(me, bit), 2)
        total = total + bit * (1 - own if d & bit else own)
        bit *= 2
    return total


def call_peers(sp_count, tp_count, sp, tp):
    barrier = pltpu.get_barrier_semaphore()
    for d in range(1, sp_count):
        pl.semaphore_signal(
            barrier, inc=1, device_id={"sp": lax.rem(sp + d, sp_count)}, device_id_type=MESH
        )
    for d in range(1, tp_count):
        pl.semaphore_signal(
            barrier, inc=1, device_id={"tp": lax.rem(tp + d, tp_count)}, device_id_type=MESH
        )


def meet_peers(sp_count, tp_count):
    pl.semaphore_wait(pltpu.get_barrier_semaphore(), sp_count + tp_count - 2)


def copy_to(src, dst, send, recv, device):
    return pltpu.make_async_remote_copy(
        src_ref=src,
        dst_ref=dst,
        send_sem=send,
        recv_sem=recv,
        device_id=device,
        device_id_type=MESH,
    )


def span(index, size):
    return pl.ds(pl.multiple_of(index * size, size), size)


def row_total(data, terms):
    ones = jnp.ones((8, data.shape[1]), BF16)
    total = None
    for _ in range(terms):
        piece = data.astype(BF16)
        data = data - piece.astype(F32)
        product = dot(ones, piece, (1, 1))
        total = product if total is None else total + product
    return total


def back(
    sp_count, tp_count, ready,
    rows_ref, switch_ref, expand_ref, contract_ref, hidden_ref, slots, weight_ref, out_ref,
    y_ref, from_sib, pair, from_peer, summed, back,
    s_sib, r_sib, s_peer, r_peer, s_back, r_back, s_own, s_fwd, r_col,
):
    sp, tp = lax.axis_index("sp"), lax.axis_index("tp")
    per, model = y_ref.shape[1:]
    rows = hidden_ref.shape[0]
    cols = model // tp_count
    mine = span(tp, cols)
    groups = tp_count // 2
    core, group = lax.rem(tp, 2), tp // 2
    sibling = group * 2 + 1 - core

    def sib_copy(s, g):
        return copy_to(
            y_ref.at[s, :, span(g * 2 + 1 - core, cols)],
            from_sib.at[s, g],
            s_sib.at[s, g],
            r_sib.at[s, g],
            {"tp": sibling},
        )

    def peer_copy(s, g):
        return copy_to(
            pair.at[s, g],
            from_peer.at[s, group],
            s_peer.at[s, g],
            r_peer.at[s, group],
            {"tp": g * 2 + core},
        )

    def back_copy(t):
        return copy_to(summed.at[t], back.at[sp], s_back.at[t], r_back.at[sp], {"sp": t})

    def others():
        return [lax.rem(group + d, groups) for d in range(1, groups)]

    local = switch_ref.shape[0]
    capacity = per // local
    chunk = math.gcd(sp_count, max(1, 256 // capacity))
    chunks = sp_count // chunk
    half = sp_count // 2
    ranks = list(range(half, sp_count)) + list(range(half - 1, -1, -1))
    order = [mate(sp, d, sp_count) for d in ranks]

    def expert(at):
        for s in at:
            ready(s)
        for e in range(local):
            inside = slice(e * capacity, (e + 1) * capacity)
            data = jnp.concatenate([rows_ref[s, inside, :] for s in at], axis=0)
            gate = dot(data, switch_ref[e])
            units = (gate / (1.0 + jnp.exp(-gate)) * dot(data, expand_ref[e])).astype(BF16)
            value = dot(units, contract_ref[e]).astype(BF16)
            for c in range(chunk):
                y_ref[at[c], inside, :] = value[c * capacity : (c + 1) * capacity]
        for s in at:
            for g in others():
                sib_copy(s, g).start()
            sib_copy(s, group).start()

    def meet(s):
        for g in others():
            sib_copy(s, g).wait_recv()
            pair[s, g] = (
                y_ref[s, :, span(g * 2 + core, cols)].astype(F32) + from_sib[s, g].astype(F32)
            ).astype(BF16)
            peer_copy(s, g).start()

    def total_up(s, own):
        sib_copy(s, group).wait_recv()
        total = y_ref[s, :, mine].astype(F32) + from_sib[s, group].astype(F32)
        for g in others():
            copy_to(
                from_peer.at[s, g],
                from_peer.at[s, g],
                s_peer.at[s, g],
                r_peer.at[s, g],
                {"tp": g * 2 + core},
            ).wait_recv()
            total = total + from_peer[s, g].astype(F32)
        if own:
            back[s] = total.astype(BF16)
        else:
            summed[s] = total.astype(BF16)
            back_copy(s).start()

    for i in range(chunks + 1):
        if i < chunks:
            at = order[i * chunk : (i + 1) * chunk]
            expert(at)
            for s in at:
                meet(s)
        if i:
            for c in range((i - 1) * chunk, i * chunk):
                total_up(order[c], ranks[c] == 0)
    weights = weight_ref[...]
    places = lax.broadcasted_iota(jnp.int32, (rows, per), 1)
    top = len(slots)
    result = hidden_ref[...]
    landing = ranks[: half - 1] + ranks[half:] + [ranks[half - 1]]
    for d in landing:
        s = mate(sp, d, sp_count)
        if d:
            copy_to(back.at[s], back.at[s], s_back.at[s], r_back.at[s], {"sp": s}).wait_recv()
        chosen = [
            jnp.where(slots[k] == places + s * per, 1.0, 0.0).astype(BF16)
            for k in range(top)
        ]
        picked = dot(stack(*chosen), back[s])
        for k in range(top):
            result = result + weights[:, k : k + 1] * picked[k * rows : (k + 1) * rows]
    out_ref[:, mine] = result.astype(BF16)

    def own_copy(p):
        here = out_ref.at[:, mine]
        return copy_to(here, here, s_own.at[p], r_col.at[tp], {"tp": p})

    def forward(o):
        here = out_ref.at[:, span(o, cols)]
        return copy_to(here, here, s_fwd.at[o], r_col.at[o], {"tp": sibling})

    peers = [g * 2 + core for g in others()]
    for p in peers:
        own_copy(p).start()
    own_copy(sibling).start()
    for p in peers:
        forward(p).wait_recv()
        forward(p).start()
    forward(sibling).wait_recv()
    for g in others():
        forward(g * 2 + 1 - core).wait_recv()
    own_copy(sibling).wait_send()
    for p in peers:
        own_copy(p).wait_send()
        forward(p).wait_send()

    def close(s, carry):
        sib_copy(s, group).wait_send()
        for g in others():
            sib_copy(s, g).wait_send()
            peer_copy(s, g).wait_send()
        return carry

    lax.fori_loop(0, sp_count, close, 0)

    def sent(d, carry):
        back_copy(lax.rem(sp + d, sp_count)).wait_send()
        return carry

    lax.fori_loop(1, sp_count, sent, 0)


def layer_kernel(
    head_dim, segment, sp_count, tp_count, experts, capacity,
    q_in, k_in, v_in, a_in, f_in, b_in, w_in, skip_in, switch_in, expand_in, contract_in,
    norm_ref, gain_ref, ids_ref, weight_ref,
    out_ref,
    q_ref, k_ref, v_ref, a_ref, f_ref, b_ref, w_ref, skip_ref, s_in,
    local, maps_in, ka, got, fold, st, mixed,
    lent, kept, from_sib, pair, from_peer, squares, outgoing,
    s_map, r_map, s_fold, r_fold, s_sib, r_sib, s_peer, r_peer,
    s_sq, r_sq, s_out, r_out, s_own, s_fwd, r_col,
    hidden_ref, rows_ref, switch_ref, expand_ref, contract_ref, *back_refs,
):
    sp, tp = lax.axis_index("sp"), lax.axis_index("tp")
    rows, channels = q_in.shape
    model = skip_in.shape[1]
    cols = model // tp_count
    width = 2 * head_dim
    heads = channels // head_dim
    share = max(1, heads // sp_count)
    workers = heads // share
    mine = span(tp, cols)
    groups = tp_count // 2
    core, group = lax.rem(tp, 2), lax.div(tp, 2)
    sibling = group * 2 + 1 - core
    others = [lax.rem(group + g, groups) for g in range(1, groups)]
    early = [
        pltpu.make_async_copy(src, dst, s_in.at[i])
        for i, (src, dst) in enumerate(
            [(f_in, f_ref), (b_in, b_ref), (k_in, k_ref), (a_in, a_ref), (q_in, q_ref),
             (v_in, v_ref), (w_in, w_ref), (skip_in, skip_ref), (switch_in, switch_ref),
             (expand_in, expand_ref), (contract_in, contract_ref)]
        )
    ]
    for copy in early:
        copy.start()
    call_peers(sp_count, tp_count, sp, tp)
    for copy in early[:6]:
        copy.wait()

    def unless_me(t, action):
        pl.when(t != sp)(action)

    def map_copy(t, owner):
        return copy_to(
            ka.at[pl.ds(t * share, share)], got.at[owner], s_map.at[t], r_map.at[owner], {"sp": t}
        )

    def fold_copy(t, owner):
        return copy_to(
            fold.at[t], st.at[pl.ds(owner * share, share)], s_fold.at[t], r_fold.at[owner], {"sp": t}
        )

    def emit_map(p, state):
        for h in range(2):
            part = slice(h * head_dim, (h + 1) * head_dim)
            ka[2 * p + h] = beside(state[:head_dim, part], state[head_dim:, part]).astype(BF16)

    def send_maps():
        meet_peers(sp_count, tp_count)
        if workers == sp_count:
            for d in range(1, sp_count):
                map_copy(mate(sp, d, sp_count), sp).start()
        else:
            for t in range(workers):
                unless_me(t, lambda t=t: map_copy(t, sp).start())

    def emit_rows(p, b, maps, out):
        at = (slice(b * segment, (b + 1) * segment), slice(p * width, (p + 1) * width))
        local[at] = out
        maps_in[at] = maps

    mixer_body(
        head_dim, segment, q_ref, k_ref, v_ref, a_ref, f_ref, b_ref, emit_map, send_maps, emit_rows
    )

    ids = ids_ref[...]
    top = ids.shape[1]
    lanes = lax.broadcasted_iota(jnp.int32, (rows, experts), 1)
    named = [ids[:, k : k + 1] == lanes for k in range(top)]
    anyone = sum(jnp.where(n, 1.0, 0.0) for n in named).astype(BF16)
    r0 = lax.broadcasted_iota(jnp.int32, (rows, rows), 0)
    r1 = lax.broadcasted_iota(jnp.int32, (rows, rows), 1)
    before = dot(jnp.where(r0 > r1, 1.0, 0.0).astype(BF16), anyone)
    slots = [
        jnp.sum(
            jnp.where(n, before + lanes.astype(F32) * capacity, 0.0), axis=1, keepdims=True
        ).astype(jnp.int32)
        for n in named
    ]
    def chain():
        got[sp] = ka[pl.ds(sp * share, share)]
        half = lax.div(lax.broadcasted_iota(jnp.int32, (head_dim, width), 1), head_dim)
        places = [half == lax.rem(sp * share + i, 2) for i in range(share)]
        state = [jnp.zeros((head_dim, head_dim), F32) for _ in range(share)]
        for j in range(sp_count):
            unless_me(
                j,
                lambda j=j: copy_to(
                    got.at[j], got.at[j], s_map.at[0], r_map.at[j], {"sp": j}
                ).wait_recv(),
            )
            for i in range(share):
                fold[j, i] = jnp.where(places[i], beside(state[i], state[i]), 0.0).astype(BF16)
            unless_me(j, lambda j=j: fold_copy(j, sp).start())
            for i in range(share):
                both = got[j, i]
                product = dot(stack(*halves(state[i])), both[:, :head_dim])
                state[i] = product[:head_dim] + product[head_dim:] + both[:, head_dim:].astype(F32)
        st[pl.ds(sp * share, share)] = fold[sp]

    if workers == sp_count:
        chain()
    else:
        pl.when(sp < workers)(chain)
    ones = jnp.where(
        lax.div(lax.broadcasted_iota(jnp.int32, (width, width), 0), head_dim)
        == lax.div(lax.broadcasted_iota(jnp.int32, (width, width), 1), head_dim),
        1.0 / head_dim,
        0.0,
    ).astype(BF16)
    ones = stack(ones, ones)
    for t in range(workers):
        unless_me(
            t,
            lambda t=t: copy_to(
                fold.at[t], st.at[pl.ds(t * share, share)], s_fold.at[0], r_fold.at[t], {"sp": t}
            ).wait_recv(),
        )
    for p in range(heads // 2):
        part = slice(p * width, (p + 1) * width)
        states = stack(st[2 * p], st[2 * p + 1])
        output = local[:, part] + dot(maps_in[:, part], states, (1, 1))
        centered = output - dot(beside(*halves(output)), ones)
        spread = dot(beside(*halves(centered * centered)), ones)
        mixed[:, part] = (centered * lax.rsqrt(spread + 0.00064) * norm_ref[:, part]).astype(BF16)

    def sib_copy(g):
        return copy_to(lent.at[g], from_sib.at[g], s_sib.at[g], r_sib.at[g], {"tp": sibling})

    def peer_copy(g):
        return copy_to(
            pair.at[g], from_peer.at[group], s_peer.at[g], r_peer.at[group], {"tp": g * 2 + core}
        )

    for copy in early[6:8]:
        copy.wait()
    for g in others + [group]:
        lent[g] = dot(mixed[...], w_ref[:, span(g * 2 + 1 - core, cols)]).astype(BF16)
        sib_copy(g).start()
    for g in others + [group]:
        kept[g] = dot(mixed[...], w_ref[:, span(g * 2 + core, cols)])
    for g in others:
        sib_copy(g).wait_recv()
        pair[g] = (kept[g] + from_sib[g].astype(F32)).astype(BF16)
        peer_copy(g).start()
    sib_copy(group).wait_recv()
    hidden = skip_ref[:, mine].astype(F32) + (kept[group] + from_sib[group].astype(F32))
    for g in others:
        copy_to(
            pair.at[g], from_peer.at[g], s_peer.at[g], r_peer.at[g], {"tp": g * 2 + core}
        ).wait_recv()
        hidden = hidden + from_peer[g].astype(F32)
    hidden_ref[...] = hidden
    squares[tp] = row_total(hidden * hidden, 3)

    def square_copy(p):
        return copy_to(squares.at[tp], squares.at[tp], s_sq.at[p], r_sq.at[tp], {"tp": p})

    for d in range(1, tp_count):
        square_copy(lax.rem(tp + d, tp_count)).start()
    total = squares[tp]
    for d in range(1, tp_count):
        p = lax.rem(tp + d, tp_count)
        copy_to(squares.at[p], squares.at[p], s_sq.at[p], r_sq.at[p], {"tp": p}).wait_recv()
        total = total + squares[p]
    inverse = lax.rsqrt(total / model + 1e-06)
    first = jnp.where(lax.broadcasted_iota(jnp.int32, (8, 128), 0) == 0, 1.0, 0.0).astype(BF16)
    column = None
    for _ in range(3):
        piece = inverse.astype(BF16)
        inverse = inverse - piece.astype(F32)
        product = dot(piece, first, (0, 0))
        column = product if column is None else column + product
    normed = (hidden * column[:, :1] * gain_ref[:, mine]).astype(BF16)

    per = experts // sp_count * capacity
    places = lax.broadcasted_iota(jnp.int32, (rows, per), 1)

    def block_for(t):
        at = places + t * per
        chosen = slots[0] == at
        for s in slots[1:]:
            chosen = chosen | (s == at)
        return dot(jnp.where(chosen, 1.0, 0.0).astype(BF16), normed, (0, 0)).astype(BF16)

    def out_copy(t):
        return copy_to(
            outgoing.at[t], rows_ref.at[sp, :, mine], s_out.at[t], r_out.at[sp], {"sp": t}
        )

    def own_copy(p, s):
        here = rows_ref.at[s, :, mine]
        return copy_to(here, here, s_own.at[p, s], r_col.at[tp, s], {"tp": p})

    def forward(o, s):
        here = rows_ref.at[s, :, span(o, cols)]
        return copy_to(here, here, s_fwd.at[o, s], r_col.at[o, s], {"tp": sibling})

    peers = [g * 2 + core for g in others]

    def pass_on(s):
        for p in peers:
            own_copy(p, s).start()
        own_copy(sibling, s).start()

    near, far = list(range(1, sp_count // 2)), list(range(sp_count // 2, sp_count))
    sending, landing = [], [0]
    for i, d in enumerate(far):
        sending += near[i : i + 1] + [d]
    landing = [0] + near[:2] + sum([[d] + near[i + 2 : i + 3] for i, d in enumerate(far)], [])
    for d in sending[:2]:
        outgoing[mate(sp, d, sp_count)] = block_for(mate(sp, d, sp_count))
        out_copy(mate(sp, d, sp_count)).start()
    rows_ref[sp, :, mine] = block_for(sp)
    pass_on(sp)
    for d in sending[2:]:
        outgoing[mate(sp, d, sp_count)] = block_for(mate(sp, d, sp_count))
        out_copy(mate(sp, d, sp_count)).start()
    lag = 2

    def relay(i):
        if i < sp_count:
            s = mate(sp, landing[i], sp_count)
            here = rows_ref.at[s, :, mine]
            copy_to(here, here, s_out.at[s], r_out.at[s], {"sp": s}).wait_recv()
            pass_on(s)
        if i >= lag:
            s = mate(sp, landing[i - lag], sp_count)
            for o in peers:
                forward(o, s).wait_recv()
                forward(o, s).start()

    def ready(s):
        forward(sibling, s).wait_recv()
        for g in others:
            forward(g * 2 + 1 - core, s).wait_recv()

    for i in range(1, sp_count + lag):
        relay(i)
    for copy in early[8:]:
        copy.wait()
    back(
        sp_count, tp_count, ready,
        rows_ref, switch_ref, expand_ref, contract_ref, hidden_ref, slots, weight_ref, out_ref,
        *back_refs,
    )

    def settle(s, carry):
        own_copy(sibling, s).wait_send()
        for p in peers:
            own_copy(p, s).wait_send()
            forward(p, s).wait_send()
        return carry

    lax.fori_loop(0, sp_count, settle, 0)

    def sent(d, carry):
        out_copy(lax.rem(sp + d, sp_count)).wait_send()
        return carry

    lax.fori_loop(1, sp_count, sent, 0)
    for d in range(1, tp_count):
        square_copy(lax.rem(tp + d, tp_count)).wait_send()
    for g in others:
        sib_copy(g).wait_send()
        peer_copy(g).wait_send()
    sib_copy(group).wait_send()
    for t in range(workers):
        unless_me(t, lambda t=t: map_copy(t, sp).wait_send())

    def folded():
        for t in range(sp_count):
            unless_me(t, lambda t=t: fold_copy(t, sp).wait_send())

    if workers == sp_count:
        folded()
    else:
        pl.when(sp < workers)(folded)


def body(
    readout_query_vectors,
    attention_key_vectors,
    attention_content_vectors,
    step_size_preactivation,
    forgetting_preactivation,
    extra_forgetting_bias,
    subspace_normalizer_gain,
    skip_connection_stream,
    blender_projection_matrix,
    specialist_prenormal_gain,
    cluster_router_chance,
    specialist_chance_within_cluster,
    chosen_specialist_ids,
    specialist_switch_matrix,
    specialist_expansion_matrix,
    specialist_contraction_matrix,
):
    tok_rows, model_width = skip_connection_stream.shape
    sp_count, tp_count = lax.axis_size("sp"), lax.axis_size("tp")
    local_experts = specialist_switch_matrix.shape[0]
    experts = local_experts * sp_count
    top_count = chosen_specialist_ids.shape[1]
    capacity = 2 * tok_rows * top_count // experts
    cols = model_width // tp_count
    per = local_experts * capacity
    groups = tp_count // 2
    channels = readout_query_vectors.shape[1]
    heads = extra_forgetting_bias.shape[1]
    head_dim = channels // heads
    share = max(1, heads // sp_count)
    vmem = pl.BlockSpec(memory_space=pltpu.VMEM)
    hbm = pl.BlockSpec(memory_space=pltpu.HBM)
    sems = pltpu.SemaphoreType.DMA
    route_weight = (
        cluster_router_chance[:, None]
        * specialist_chance_within_cluster
        / jnp.sum(specialist_chance_within_cluster, axis=1, keepdims=True)
    )
    return pl.pallas_call(
        functools.partial(
            layer_kernel, head_dim, min(64, tok_rows), sp_count, tp_count, experts, capacity
        ),
        out_shape=jax.ShapeDtypeStruct((tok_rows, model_width), BF16),
        in_specs=[hbm] * 11 + [vmem] * 4,
        out_specs=vmem,
        scratch_shapes=[
            pltpu.VMEM((tok_rows, channels), BF16),
            pltpu.VMEM((tok_rows, channels), BF16),
            pltpu.VMEM((tok_rows, channels), BF16),
            pltpu.VMEM((tok_rows, channels), BF16),
            pltpu.VMEM((tok_rows, channels), F32),
            pltpu.VMEM((heads, tok_rows), F32),
            pltpu.VMEM((channels, model_width), BF16),
            pltpu.VMEM((tok_rows, model_width), BF16),
            sems((11,)),
            pltpu.VMEM((tok_rows, channels), F32),
            pltpu.VMEM((tok_rows, channels), BF16),
            pltpu.VMEM((heads, head_dim, 2 * head_dim), BF16),
            pltpu.VMEM((sp_count, share, head_dim, 2 * head_dim), BF16),
            pltpu.VMEM((sp_count, share, head_dim, 2 * head_dim), BF16),
            pltpu.VMEM((heads, head_dim, 2 * head_dim), BF16),
            pltpu.VMEM((tok_rows, channels), BF16),
            pltpu.VMEM((groups, tok_rows, cols), BF16),
            pltpu.VMEM((groups, tok_rows, cols), F32),
            pltpu.VMEM((groups, tok_rows, cols), BF16),
            pltpu.VMEM((groups, tok_rows, cols), BF16),
            pltpu.VMEM((groups, tok_rows, cols), BF16),
            pltpu.VMEM((tp_count, 8, tok_rows), F32),
            pltpu.VMEM((sp_count, per, cols), BF16),
            sems((sp_count,)),
            sems((sp_count,)),
            sems((sp_count,)),
            sems((sp_count,)),
            sems((groups,)),
            sems((groups,)),
            sems((groups,)),
            sems((groups,)),
            sems((tp_count,)),
            sems((tp_count,)),
            sems((sp_count,)),
            sems((sp_count,)),
            sems((tp_count, sp_count)),
            sems((tp_count, sp_count)),
            sems((tp_count, sp_count)),
            pltpu.VMEM((tok_rows, cols), F32),
            pltpu.VMEM((sp_count, per, model_width), BF16),
            pltpu.VMEM(specialist_switch_matrix.shape, BF16),
            pltpu.VMEM(specialist_expansion_matrix.shape, BF16),
            pltpu.VMEM(specialist_contraction_matrix.shape, BF16),
            pltpu.VMEM((sp_count, per, model_width), BF16),
            pltpu.VMEM((sp_count, groups, per, cols), BF16),
            pltpu.VMEM((sp_count, groups, per, cols), BF16),
            pltpu.VMEM((sp_count, groups, per, cols), BF16),
            pltpu.VMEM((sp_count, per, cols), BF16),
            pltpu.VMEM((sp_count, per, cols), BF16),
            sems((sp_count, groups)),
            sems((sp_count, groups)),
            sems((sp_count, groups)),
            sems((sp_count, groups)),
            sems((sp_count,)),
            sems((sp_count,)),
            sems((tp_count,)),
            sems((tp_count,)),
            sems((tp_count,)),
        ],
        compiler_params=pltpu.CompilerParams(
            collective_id=1, has_side_effects=True, vmem_limit_bytes=VMEM_LIMIT
        ),
    )(
        readout_query_vectors,
        attention_key_vectors,
        attention_content_vectors,
        step_size_preactivation,
        forgetting_preactivation,
        extra_forgetting_bias.T,
        blender_projection_matrix,
        skip_connection_stream,
        specialist_switch_matrix,
        specialist_expansion_matrix,
        specialist_contraction_matrix,
        subspace_normalizer_gain.reshape(1, channels),
        specialist_prenormal_gain.reshape(1, model_width),
        chosen_specialist_ids,
        route_weight,
    )


def solution(mesh):
    in_specs = (
        P("sp", "tp"),
        P("sp", "tp"),
        P("sp", "tp"),
        P("sp", "tp"),
        P("sp", "tp"),
        P("sp", "tp"),
        P("tp"),
        P("sp", None),
        P("tp", None),
        P(),
        P("sp"),
        P("sp", None),
        P("sp", None),
        P("sp", None, "tp"),
        P("sp", None, "tp"),
        P("sp", "tp", None),
    )
    out_specs = P("sp", None)
    return jax.shard_map(body, mesh=mesh, in_specs=in_specs, out_specs=out_specs, check_vma=False)
```

```python
import functools
import math

import jax
import jax.numpy as jnp
from jax import lax
from jax.experimental import pallas as pl
from jax.experimental.pallas import tpu as pltpu
from jax.sharding import PartitionSpec as P

MESH = pl.DeviceIdType.MESH
F32 = jnp.float32
BF16 = jnp.bfloat16
VMEM_LIMIT = 63 * 1024 * 1024
SENDS = [6, 1, 5, 2, 3, 4, 7]
SCRIPT = [
    ("R", 1), ("R", 0), ("R", 6), ("R", 5), ("R", 2), ("R", 3), ("F", 5), ("F", 0), ("F", 2),
    ("R", 4), ("E", 2, 5), ("F", 3), ("M", 5), ("E", 3), ("F", 1), ("F", 4), ("R", 7), ("M", 3),
    ("F", 6), ("E", 4), ("E", 1), ("M", 4), ("T", 5), ("F", 7), ("M", 2), ("E", 7, 0), ("T", 3),
    ("E", 6), ("M", 7), ("T", 4), ("T", 7), ("M", 6), ("C", 3), ("M", 1), ("T", 2), ("T", 6),
    ("M", 0), ("T", 1), ("C", 2), ("T", 0), ("C", 5), ("C", 1), ("C", 0), ("C", 4), ("C", 7),
    ("C", 6),
]


def dot(left, right, axes=(1, 0)):
    return lax.dot_general(
        left, right, (((axes[0],), (axes[1],)), ((), ())), preferred_element_type=F32
    )


def halves(data):
    high = data.astype(BF16)
    return high, (data - high.astype(F32)).astype(BF16)


def stack(*parts):
    return jnp.concatenate(parts, axis=0)


def beside(*parts):
    return jnp.concatenate(parts, axis=1)


def mixer_setup(head_dim, segment, pairs):
    width = 2 * head_dim
    row = lax.broadcasted_iota(jnp.int32, (segment, width), 0)
    lane = lax.broadcasted_iota(jnp.int32, (segment, width), 1)
    col = lane & (segment - 1)
    return row, lane, col


def split_pair(head_dim):
    def pick(data):
        lane = lax.broadcasted_iota(jnp.int32, data.shape, 1)
        zero = jnp.zeros_like(data)
        return stack(jnp.where(lane < head_dim, data, zero), jnp.where(lane < head_dim, zero, data))

    return pick


def thirds(data):
    high = data.astype(BF16)
    rest = data - high.astype(F32)
    middle = rest.astype(BF16)
    return high, middle, (rest - middle.astype(F32)).astype(BF16)


def mixer_body(head_dim, segment, q_ref, k_ref, v_ref, a_ref, f_ref, b_ref, emit_map, between, emit_rows):
    rows, channels = q_ref.shape
    width = 2 * head_dim
    pairs = channels // width
    heads = channels // head_dim
    blocks = rows // segment
    shift = segment.bit_length() - 1
    row, lane, col = mixer_setup(head_dim, segment, pairs)
    strict, inclusive = row > col, row >= col
    bd = split_pair(head_dim)
    own = lax.broadcasted_iota(jnp.int32, (width, width), 0) // head_dim == (
        lax.broadcasted_iota(jnp.int32, (width, width), 1) // head_dim
    )
    ones = jnp.where(own, 1.0, 0.0).astype(BF16)
    ones = stack(ones, ones)
    spread = jnp.where(
        lax.rem(lax.broadcasted_iota(jnp.int32, (3 * heads, channels), 0), heads)
        == lax.broadcasted_iota(jnp.int32, (3 * heads, channels), 1) // head_dim,
        1.0,
        0.0,
    ).astype(BF16)
    pieces = stack(*[piece.astype(F32) for piece in thirds(b_ref[...])]).astype(BF16)
    bias = dot(pieces, spread, (0, 0))
    t0 = lax.broadcasted_iota(jnp.int32, (segment, segment), 0)
    t1 = lax.broadcasted_iota(jnp.int32, (segment, segment), 1)
    triangle = jnp.where(t0 >= t1, 1.0, 0.0).astype(BF16)
    triangle = beside(triangle, triangle, triangle)
    chains = [(p, b) for p in range(pairs) for b in range(blocks)]

    def prepare(p, b):
        at = (slice(b * segment, (b + 1) * segment), slice(p * width, (p + 1) * width))
        decay = -(0.6065306597126334 / (1.0 + jnp.exp(-f_ref[at]))) + bias[at]
        cumulative = dot(triangle, stack(*thirds(decay)))
        keys = k_ref[at].astype(F32)
        norms = dot(beside(*halves(keys * keys)), ones)
        removal = keys * lax.rsqrt(norms + 1e-06)
        beta = removal * (1.0 / (1.0 + jnp.exp(-a_ref[at].astype(F32))))
        closing = cumulative[segment - 1 :, :]
        grow = jnp.exp(-cumulative)
        fade = jnp.exp(closing - cumulative)
        c = {}
        c["alpha"] = -removal * jnp.exp(cumulative - decay)
        c["query"] = q_ref[at].astype(F32) * jnp.exp(cumulative)
        c["beta_hat"] = beta * grow
        c["key_hat"] = (keys * grow).astype(BF16)
        c["beta_bar"] = beta * fade
        c["key_bar"] = (keys * fade).astype(BF16)
        c["keep"] = jnp.where(row == col, jnp.exp(closing), 0.0)
        c["values"] = v_ref[at]
        return c

    C = [prepare(p, b) for p, b in chains]

    for c in C:
        ah, al = halves(c["alpha"])
        bh, bl = halves(c["beta_hat"])
        qh = c["query"].astype(BF16)
        by_beta = dot(stack(ah, al, qh), bd(bh), (1, 1))
        low = dot(ah, bd(bl), (1, 1))
        by_key = dot(stack(ah, qh), bd(c["key_hat"]), (1, 1))
        c["lower"] = jnp.where(strict, by_beta[:segment] + by_beta[segment : 2 * segment] + low, 0.0)
        c["read_remove"] = jnp.where(inclusive, by_beta[2 * segment :], 0.0).astype(BF16)
        c["remove_write"] = jnp.where(strict, by_key[:segment], 0.0)
        c["read_write"] = jnp.where(inclusive, by_key[segment:], 0.0).astype(BF16)
        c["ah"] = ah
        c["lh"], c["ll"] = halves(c["lower"])
    for c in C:
        wh, wl = halves(c["remove_write"])
        product = dot(stack(wh, wl, c["read_write"]), bd(c["values"]))
        c["side"] = product[:segment] + product[segment : 2 * segment]
        c["local"] = product[2 * segment :]
        c["inverse"] = jnp.where(
            row == col, 1.0, jnp.where((row >> 1) == (col >> 1), c["lower"], 0.0)
        )
    zero = jnp.zeros((segment, width), BF16)
    for s in range(1, shift):
        off = ((row >> (s + 1)) == (col >> (s + 1))) & ((row >> s) != (col >> s))
        for c in C:
            c["near"] = c["inverse"].astype(BF16)
            c["reach"] = dot(jnp.where(off, c["lh"], zero), bd(c["near"]))
        for c in C:
            c["inverse"] = c["inverse"] + dot(c["near"], bd(c["reach"].astype(BF16)))
    for c in C:
        c["near"] = c["inverse"].astype(BF16)
        c["both"] = beside(c["alpha"], c["side"])
        c["solved"] = dot(c["near"], beside(bd(c["ah"]), bd(c["side"].astype(BF16))))
    for c in C:
        sh, sl = halves(c["solved"])
        high = dot(stack(c["lh"], c["ll"]), beside(bd(sh[:, :width]), bd(sh[:, width:])))
        low = dot(c["lh"], beside(bd(sl[:, :width]), bd(sl[:, width:])))
        c["miss"] = c["both"] - c["solved"] + (high[:segment] + (high[segment:] + low))
    for c in C:
        miss = c["miss"].astype(BF16)
        c["solved"] = c["solved"] + dot(c["near"], beside(bd(miss[:, :width]), bd(miss[:, width:])))
    for c in C:
        sh, sl = halves(c["solved"])
        c["sh"] = sh
        bh, bl = halves(c["beta_bar"])
        left = stack(sh, sl, sh, beside(zero, c["values"]))
        step = dot(left, stack(bh, bh, bl, c["key_bar"]), (0, 0))
        first = lane < head_dim
        c["keep"] = c["keep"] + jnp.where(first, step[:head_dim], step[head_dim:width])
        c["add"] = jnp.where(first, step[width : width + head_dim], step[width + head_dim :])
    states = [[None] for _ in range(pairs)]
    now = [stack(C[p * blocks]["keep"], C[p * blocks]["add"]) for p in range(pairs)]
    for b in range(1, blocks):
        for p in range(pairs):
            c = C[p * blocks + b]
            kh, kl = halves(c["keep"])
            th, tl = halves(now[p])
            states[p].append(th)
            high = dot(stack(th, tl), bd(kh))
            low = dot(th, bd(kl))
            total = high[:width] + (high[width:] + low)
            now[p] = stack(total[:head_dim], total[head_dim:] + c["add"])
    for p in range(pairs):
        emit_map(p, now[p])
    between()
    for i, (p, b) in enumerate(chains):
        c = C[i]
        sh = c["sh"]
        read = dot(c["read_remove"], beside(bd(sh[:, :width]), bd(sh[:, width:])))
        c["read_map"] = c["query"] + read[:, :width]
        c["local"] = c["local"] + read[:, width:]
    for i, (p, b) in enumerate(chains):
        c = C[i]
        maps, local = c["read_map"].astype(BF16), c["local"]
        if b:
            th = states[p][b]
            seen = dot(maps, stack(bd(th[:head_dim]), bd(th[head_dim:])), (1, 1))
            maps, local = seen[:, :width].astype(BF16), local + seen[:, width:]
        emit_rows(p, b, maps, local)


def mate(me, d, count):
    total, bit = 0, 1
    while bit < count:
        own = lax.rem(lax.div(me, bit), 2)
        total = total + bit * (1 - own if d & bit else own)
        bit *= 2
    return total


def call_peers(sp_count, tp_count, sp, tp):
    barrier = pltpu.get_barrier_semaphore()
    for d in range(1, sp_count):
        pl.semaphore_signal(
            barrier, inc=1, device_id={"sp": lax.rem(sp + d, sp_count)}, device_id_type=MESH
        )
    for d in range(1, tp_count):
        pl.semaphore_signal(
            barrier, inc=1, device_id={"tp": lax.rem(tp + d, tp_count)}, device_id_type=MESH
        )


def meet_peers(sp_count, tp_count):
    pl.semaphore_wait(pltpu.get_barrier_semaphore(), sp_count + tp_count - 2)


def copy_to(src, dst, send, recv, device):
    return pltpu.make_async_remote_copy(
        src_ref=src,
        dst_ref=dst,
        send_sem=send,
        recv_sem=recv,
        device_id=device,
        device_id_type=MESH,
    )


def span(index, size):
    return pl.ds(pl.multiple_of(index * size, size), size)


def row_total(data, terms):
    ones = jnp.ones((8, data.shape[1]), BF16)
    total = None
    for _ in range(terms):
        piece = data.astype(BF16)
        data = data - piece.astype(F32)
        product = dot(ones, piece, (1, 1))
        total = product if total is None else total + product
    return total


def experts_back(
    sp_count, tp_count, ready,
    rows_ref, switch_ref, expand_ref, contract_ref, hidden_ref, slots, weights,
    y_ref, from_sib, pair, from_peer, summed, back,
    s_sib, r_sib, s_peer, r_peer, s_back, r_back, ending,
):
    sp, tp = lax.axis_index("sp"), lax.axis_index("tp")
    per, model = y_ref.shape[1:]
    rows = hidden_ref.shape[0]
    cols = model // tp_count
    mine = span(tp, cols)
    groups = tp_count // 2
    core, group = lax.rem(tp, 2), lax.div(tp, 2)
    sibling = group * 2 + 1 - core
    others = [lax.rem(group + d, groups) for d in range(1, groups)]
    local = switch_ref.shape[0]
    capacity = per // local
    top = len(slots)
    places = lax.broadcasted_iota(jnp.int32, (rows, per), 1)

    def sib_copy(s, g):
        return copy_to(
            y_ref.at[s, :, span(g * 2 + 1 - core, cols)],
            from_sib.at[s, g],
            s_sib.at[s, g],
            r_sib.at[s, g],
            {"tp": sibling},
        )

    def peer_copy(s, g):
        return copy_to(
            pair.at[s, g],
            from_peer.at[s, group],
            s_peer.at[s, g],
            r_peer.at[s, group],
            {"tp": g * 2 + core},
        )

    def back_copy(t):
        return copy_to(summed.at[t], back.at[sp], s_back.at[t], r_back.at[sp], {"sp": t})

    def close(s, carry):
        sib_copy(s, group).wait_send()
        for g in others:
            sib_copy(s, g).wait_send()
            peer_copy(s, g).wait_send()
        return carry

    def sent(d, carry):
        back_copy(lax.rem(sp + d, sp_count)).wait_send()
        return carry

    ending.append(lambda: lax.fori_loop(0, sp_count, close, 0))
    ending.append(lambda: lax.fori_loop(1, sp_count, sent, 0))

    def expert(at):
        for s in at:
            ready(s)
        for e in range(local):
            inside = slice(e * capacity, (e + 1) * capacity)
            data = jnp.concatenate([rows_ref[s, inside, :] for s in at], axis=0)
            gate = dot(data, switch_ref[e])
            units = (gate / (1.0 + jnp.exp(-gate)) * dot(data, expand_ref[e])).astype(BF16)
            value = dot(units, contract_ref[e]).astype(BF16)
            for c, s in enumerate(at):
                y_ref[s, inside, :] = value[c * capacity : (c + 1) * capacity]
        for s in at:
            for g in others:
                sib_copy(s, g).start()
            sib_copy(s, group).start()

    def meet(s):
        for g in others:
            sib_copy(s, g).wait_recv()
            pair[s, g] = (
                y_ref[s, :, span(g * 2 + core, cols)].astype(F32) + from_sib[s, g].astype(F32)
            ).astype(BF16)
            peer_copy(s, g).start()

    def total_up(s, own):
        sib_copy(s, group).wait_recv()
        total = y_ref[s, :, mine].astype(F32) + from_sib[s, group].astype(F32)
        for g in others:
            copy_to(
                from_peer.at[s, g],
                from_peer.at[s, g],
                s_peer.at[s, g],
                r_peer.at[s, g],
                {"tp": g * 2 + core},
            ).wait_recv()
            total = total + from_peer[s, g].astype(F32)
        if own:
            back[s] = total.astype(BF16)
        else:
            summed[s] = total.astype(BF16)
            back_copy(s).start()

    def combine(s, own):
        if not own:
            copy_to(back.at[s], back.at[s], s_back.at[s], r_back.at[s], {"sp": s}).wait_recv()
        chosen = [
            jnp.where(slots[k] == places + s * per, 1.0, 0.0).astype(BF16) for k in range(top)
        ]
        picked = dot(stack(*chosen), back[s])
        total = hidden_ref[...]
        for k in range(top):
            total = total + weights[k] * picked[k * rows : (k + 1) * rows]
        hidden_ref[...] = total

    return expert, meet, total_up, combine


def gather_out(tp_count, hidden_ref, out_ref, s_own, s_fwd, r_col):
    tp = lax.axis_index("tp")
    model = out_ref.shape[1]
    cols = model // tp_count
    mine = span(tp, cols)
    groups = tp_count // 2
    core, group = lax.rem(tp, 2), lax.div(tp, 2)
    sibling = group * 2 + 1 - core
    others = [lax.rem(group + d, groups) for d in range(1, groups)]
    out_ref[:, mine] = hidden_ref[...].astype(BF16)

    def own_copy(p):
        here = out_ref.at[:, mine]
        return copy_to(here, here, s_own.at[p], r_col.at[tp], {"tp": p})

    def forward(o):
        here = out_ref.at[:, span(o, cols)]
        return copy_to(here, here, s_fwd.at[o], r_col.at[o], {"tp": sibling})

    peers = [g * 2 + core for g in others]
    for p in peers:
        own_copy(p).start()
    own_copy(sibling).start()
    for p in peers:
        forward(p).wait_recv()
        forward(p).start()
    forward(sibling).wait_recv()
    for g in others:
        forward(g * 2 + 1 - core).wait_recv()
    own_copy(sibling).wait_send()
    for p in peers:
        own_copy(p).wait_send()
        forward(p).wait_send()


def plan(count, capacity):
    half = count // 2
    near, far = list(range(half)), list(range(half, count))
    if count == 8 and capacity == 128:
        return SENDS, SCRIPT
    chunk = max(1, 256 // capacity)
    steps = []
    for d in near + far:
        steps += [("R", d), ("F", d)]
    ranks = far + near[::-1]
    for i in range(0, count, chunk):
        steps.append(("E", *ranks[i : i + chunk]))
        steps += [("M", d) for d in ranks[i : i + chunk]]
        steps += [("T", d) for d in ranks[i : i + chunk]]
    return near[1:] + far, steps + [("C", d) for d in ranks]


def layer_kernel(
    head_dim, segment, sp_count, tp_count, experts, capacity,
    q_in, k_in, v_in, a_in, f_in, b_in, w_in, skip_in, switch_in, expand_in, contract_in,
    norm_in, gain_in, ids_in, chance_in, within_in,
    out_ref,
    q_ref, k_ref, v_ref, a_ref, f_ref, b_ref, w_ref, skip_ref,
    norm_ref, gain_ref, ids_ref, chance_ref, within_ref, s_in,
    local, maps_in, ka, got, fold, st, mixed,
    lent, kept, from_sib, pair, from_peer, squares, outgoing,
    s_map, r_map, s_fold, r_fold, s_sib, r_sib, s_peer, r_peer,
    s_sq, r_sq, s_out, r_out, s_own, s_fwd, r_col,
    hidden_ref, rows_ref, switch_ref, expand_ref, contract_ref, *back_refs,
):
    sp, tp = lax.axis_index("sp"), lax.axis_index("tp")
    rows, channels = q_in.shape
    model = skip_in.shape[1]
    cols = model // tp_count
    width = 2 * head_dim
    heads = channels // head_dim
    share = max(1, heads // sp_count)
    workers = heads // share
    mine = span(tp, cols)
    groups = tp_count // 2
    core, group = lax.rem(tp, 2), lax.div(tp, 2)
    sibling = group * 2 + 1 - core
    others = [lax.rem(group + g, groups) for g in range(1, groups)]
    early = [
        pltpu.make_async_copy(src, dst, s_in.at[i])
        for i, (src, dst) in enumerate(
            [(f_in, f_ref), (b_in, b_ref), (k_in, k_ref), (a_in, a_ref), (q_in, q_ref),
             (v_in, v_ref), (norm_in, norm_ref), (gain_in, gain_ref), (ids_in, ids_ref),
             (chance_in, chance_ref), (within_in, within_ref), (w_in, w_ref),
             (skip_in, skip_ref), (switch_in, switch_ref), (expand_in, expand_ref),
             (contract_in, contract_ref)]
        )
    ]
    for copy in early[:6]:
        copy.start()
    call_peers(sp_count, tp_count, sp, tp)
    for copy in early[:6]:
        copy.wait()
    for copy in early[6:]:
        copy.start()
    ending = []

    def unless_me(t, action):
        pl.when(t != sp)(action)

    def map_copy(t, owner):
        return copy_to(
            ka.at[pl.ds(t * share, share)], got.at[owner], s_map.at[t], r_map.at[owner], {"sp": t}
        )

    def fold_copy(t, owner):
        return copy_to(
            fold.at[t], st.at[pl.ds(owner * share, share)], s_fold.at[t], r_fold.at[owner], {"sp": t}
        )

    def emit_map(p, state):
        for h in range(2):
            part = slice(h * head_dim, (h + 1) * head_dim)
            ka[2 * p + h] = beside(state[:head_dim, part], state[head_dim:, part]).astype(BF16)

    def send_maps():
        meet_peers(sp_count, tp_count)
        if workers == sp_count:
            for d in range(1, sp_count):
                map_copy(mate(sp, d, sp_count), sp).start()
        else:
            for t in range(workers):
                unless_me(t, lambda t=t: map_copy(t, sp).start())

    def emit_rows(p, b, maps, out):
        at = (slice(b * segment, (b + 1) * segment), slice(p * width, (p + 1) * width))
        local[at] = out
        maps_in[at] = maps

    mixer_body(
        head_dim, segment, q_ref, k_ref, v_ref, a_ref, f_ref, b_ref, emit_map, send_maps, emit_rows
    )

    for copy in early[6:]:
        copy.wait()
    top = ids_ref.shape[0]
    within = within_ref[...]
    shares = chance_ref[...] * within / jnp.sum(within, axis=0, keepdims=True)
    lines = [ids_ref[k : k + 1, :].astype(F32) for k in range(top)]
    lines = lines + [shares[k : k + 1, :] for k in range(top)]
    place = lax.broadcasted_iota(jnp.int32, (8, rows), 0)
    table = jnp.zeros((8, rows), F32)
    for k in range(2 * top):
        table = jnp.where(place == k, lines[k], table)
    pieces = stack(*[piece.astype(F32) for piece in thirds(table)]).astype(BF16)
    unit = jnp.where(
        lax.rem(lax.broadcasted_iota(jnp.int32, (24, 128), 0), 8)
        == lax.broadcasted_iota(jnp.int32, (24, 128), 1),
        1.0,
        0.0,
    ).astype(BF16)
    upright = dot(pieces, unit, (0, 0))
    weights = [upright[:, top + k : top + k + 1] for k in range(top)]
    lanes = lax.broadcasted_iota(jnp.int32, (rows, experts), 1).astype(F32)
    named = [upright[:, k : k + 1] == lanes for k in range(top)]
    anyone = sum(jnp.where(n, 1.0, 0.0) for n in named).astype(BF16)
    r0 = lax.broadcasted_iota(jnp.int32, (rows, rows), 0)
    r1 = lax.broadcasted_iota(jnp.int32, (rows, rows), 1)
    before = dot(jnp.where(r0 > r1, 1.0, 0.0).astype(BF16), anyone)
    slots = [
        jnp.sum(
            jnp.where(n, before + lanes * capacity, 0.0), axis=1, keepdims=True
        ).astype(jnp.int32)
        for n in named
    ]
    def chain():
        got[sp] = ka[pl.ds(sp * share, share)]
        half = lax.div(lax.broadcasted_iota(jnp.int32, (head_dim, width), 1), head_dim)
        places = [half == lax.rem(sp * share + i, 2) for i in range(share)]
        state = [jnp.zeros((head_dim, head_dim), F32) for _ in range(share)]
        for j in range(sp_count):
            unless_me(
                j,
                lambda j=j: copy_to(
                    got.at[j], got.at[j], s_map.at[0], r_map.at[j], {"sp": j}
                ).wait_recv(),
            )
            for i in range(share):
                fold[j, i] = jnp.where(places[i], beside(state[i], state[i]), 0.0).astype(BF16)
            unless_me(j, lambda j=j: fold_copy(j, sp).start())
            for i in range(share):
                both = got[j, i]
                product = dot(stack(*halves(state[i])), both[:, :head_dim])
                state[i] = product[:head_dim] + product[head_dim:] + both[:, head_dim:].astype(F32)
        st[pl.ds(sp * share, share)] = fold[sp]

    def map_sent():
        for t in range(workers):
            unless_me(t, lambda t=t: map_copy(t, sp).wait_send())

    def fold_sent():
        for t in range(sp_count):
            unless_me(t, lambda t=t: fold_copy(t, sp).wait_send())

    ending.append(map_sent)
    ending.append(fold_sent if workers == sp_count else lambda: pl.when(sp < workers)(fold_sent))
    if workers == sp_count:
        chain()
    else:
        pl.when(sp < workers)(chain)
    ones = jnp.where(
        lax.div(lax.broadcasted_iota(jnp.int32, (width, width), 0), head_dim)
        == lax.div(lax.broadcasted_iota(jnp.int32, (width, width), 1), head_dim),
        1.0 / head_dim,
        0.0,
    ).astype(BF16)
    ones = stack(ones, ones)
    for t in range(workers):
        unless_me(
            t,
            lambda t=t: copy_to(
                fold.at[t], st.at[pl.ds(t * share, share)], s_fold.at[0], r_fold.at[t], {"sp": t}
            ).wait_recv(),
        )
    for p in range(heads // 2):
        part = slice(p * width, (p + 1) * width)
        states = stack(st[2 * p], st[2 * p + 1])
        output = local[:, part] + dot(maps_in[:, part], states, (1, 1))
        centered = output - dot(beside(*halves(output)), ones)
        spread = dot(beside(*halves(centered * centered)), ones)
        mixed[:, part] = (centered * lax.rsqrt(spread + 0.00064) * norm_ref[:, part]).astype(BF16)

    def sib_copy(g):
        return copy_to(lent.at[g], from_sib.at[g], s_sib.at[g], r_sib.at[g], {"tp": sibling})

    def peer_copy(g):
        return copy_to(
            pair.at[g], from_peer.at[group], s_peer.at[g], r_peer.at[group], {"tp": g * 2 + core}
        )

    ending.append(lambda: [sib_copy(g).wait_send() for g in others + [group]])
    ending.append(lambda: [peer_copy(g).wait_send() for g in others])
    for g in others + [group]:
        lent[g] = dot(mixed[...], w_ref[:, span(g * 2 + 1 - core, cols)]).astype(BF16)
        sib_copy(g).start()
    for g in others + [group]:
        kept[g] = dot(mixed[...], w_ref[:, span(g * 2 + core, cols)])
    for g in others:
        sib_copy(g).wait_recv()
        pair[g] = (kept[g] + from_sib[g].astype(F32)).astype(BF16)
        peer_copy(g).start()
    sib_copy(group).wait_recv()
    hidden = skip_ref[:, mine].astype(F32) + (kept[group] + from_sib[group].astype(F32))
    for g in others:
        copy_to(
            pair.at[g], from_peer.at[g], s_peer.at[g], r_peer.at[g], {"tp": g * 2 + core}
        ).wait_recv()
        hidden = hidden + from_peer[g].astype(F32)
    hidden_ref[...] = hidden
    squares[tp] = row_total(hidden * hidden, 3)

    def square_copy(p):
        return copy_to(squares.at[tp], squares.at[tp], s_sq.at[p], r_sq.at[tp], {"tp": p})

    ending.append(
        lambda: [square_copy(lax.rem(tp + d, tp_count)).wait_send() for d in range(1, tp_count)]
    )
    for d in range(1, tp_count):
        square_copy(lax.rem(tp + d, tp_count)).start()
    total = squares[tp]
    for d in range(1, tp_count):
        p = lax.rem(tp + d, tp_count)
        copy_to(squares.at[p], squares.at[p], s_sq.at[p], r_sq.at[p], {"tp": p}).wait_recv()
        total = total + squares[p]
    inverse = lax.rsqrt(total / model + 1e-06)
    first = jnp.where(lax.broadcasted_iota(jnp.int32, (8, 128), 0) == 0, 1.0, 0.0).astype(BF16)
    column = None
    for _ in range(3):
        piece = inverse.astype(BF16)
        inverse = inverse - piece.astype(F32)
        product = dot(piece, first, (0, 0))
        column = product if column is None else column + product
    normed = (hidden * column[:, :1] * gain_ref[:, mine]).astype(BF16)

    per = experts // sp_count * capacity
    places = lax.broadcasted_iota(jnp.int32, (rows, per), 1)

    def block_for(t):
        at = places + t * per
        chosen = slots[0] == at
        for s in slots[1:]:
            chosen = chosen | (s == at)
        return dot(jnp.where(chosen, 1.0, 0.0).astype(BF16), normed, (0, 0)).astype(BF16)

    def out_copy(t):
        return copy_to(
            outgoing.at[t], rows_ref.at[sp, :, mine], s_out.at[t], r_out.at[sp], {"sp": t}
        )

    def own_copy(p, s):
        here = rows_ref.at[s, :, mine]
        return copy_to(here, here, s_own.at[p, s], r_col.at[tp, s], {"tp": p})

    def forward(o, s):
        here = rows_ref.at[s, :, span(o, cols)]
        return copy_to(here, here, s_fwd.at[o, s], r_col.at[o, s], {"tp": sibling})

    peers = [g * 2 + core for g in others]

    def pass_on(s):
        for p in peers:
            own_copy(p, s).start()
        own_copy(sibling, s).start()

    def settle(s, carry):
        own_copy(sibling, s).wait_send()
        for p in peers:
            own_copy(p, s).wait_send()
            forward(p, s).wait_send()
        return carry

    def sent(d, carry):
        out_copy(lax.rem(sp + d, sp_count)).wait_send()
        return carry

    ending.append(lambda: lax.fori_loop(0, sp_count, settle, 0))
    ending.append(lambda: lax.fori_loop(1, sp_count, sent, 0))
    def ready(s):
        forward(sibling, s).wait_recv()
        for g in others:
            forward(g * 2 + 1 - core, s).wait_recv()

    sends, steps = plan(sp_count, capacity)

    def source(d):
        return mate(sp, d, sp_count)

    y_ref, sib_back, pair_back, peer_back, summed, returned = back_refs[:6]
    s_sib2, r_sib2, s_peer2, r_peer2, s_back, r_back, s_last, s_fwd2, r_last = back_refs[6:]
    for d in sends:
        t = mate(sp, d, sp_count)
        outgoing[t] = block_for(t)
        out_copy(t).start()
    rows_ref[sp, :, mine] = block_for(sp)
    expert, meet, total_up, combine = experts_back(
        sp_count, tp_count, ready,
        rows_ref, switch_ref, expand_ref, contract_ref, hidden_ref, slots, weights,
        y_ref, sib_back, pair_back, peer_back, summed, returned,
        s_sib2, r_sib2, s_peer2, r_peer2, s_back, r_back, ending,
    )
    for kind, *which in steps:
        for d in which[:1] if kind == "E" else which:
            s = source(d)
            if kind == "R":
                if d:
                    here = rows_ref.at[s, :, mine]
                    copy_to(here, here, s_out.at[s], r_out.at[s], {"sp": s}).wait_recv()
                pass_on(s)
            if kind == "F":
                for o in peers:
                    forward(o, s).wait_recv()
                    forward(o, s).start()
            if kind == "E":
                expert([source(i) for i in which])
            if kind == "M":
                meet(s)
            if kind == "T":
                total_up(s, d == 0)
            if kind == "C":
                combine(s, d == 0)
    gather_out(tp_count, hidden_ref, out_ref, s_last, s_fwd2, r_last)
    for wait in ending:
        wait()


def body(
    readout_query_vectors,
    attention_key_vectors,
    attention_content_vectors,
    step_size_preactivation,
    forgetting_preactivation,
    extra_forgetting_bias,
    subspace_normalizer_gain,
    skip_connection_stream,
    blender_projection_matrix,
    specialist_prenormal_gain,
    cluster_router_chance,
    specialist_chance_within_cluster,
    chosen_specialist_ids,
    specialist_switch_matrix,
    specialist_expansion_matrix,
    specialist_contraction_matrix,
):
    tok_rows, model_width = skip_connection_stream.shape
    sp_count, tp_count = lax.axis_size("sp"), lax.axis_size("tp")
    local_experts = specialist_switch_matrix.shape[0]
    experts = local_experts * sp_count
    top_count = chosen_specialist_ids.shape[1]
    capacity = 2 * tok_rows * top_count // experts
    cols = model_width // tp_count
    per = local_experts * capacity
    groups = tp_count // 2
    channels = readout_query_vectors.shape[1]
    heads = extra_forgetting_bias.shape[1]
    head_dim = channels // heads
    share = max(1, heads // sp_count)
    vmem = pl.BlockSpec(memory_space=pltpu.VMEM)
    hbm = pl.BlockSpec(memory_space=pltpu.HBM)
    sems = pltpu.SemaphoreType.DMA
    return pl.pallas_call(
        functools.partial(
            layer_kernel, head_dim, min(64, tok_rows), sp_count, tp_count, experts, capacity
        ),
        out_shape=jax.ShapeDtypeStruct((tok_rows, model_width), BF16),
        in_specs=[hbm] * 16,
        out_specs=vmem,
        scratch_shapes=[
            pltpu.VMEM((tok_rows, channels), BF16),
            pltpu.VMEM((tok_rows, channels), BF16),
            pltpu.VMEM((tok_rows, channels), BF16),
            pltpu.VMEM((tok_rows, channels), BF16),
            pltpu.VMEM((tok_rows, channels), F32),
            pltpu.VMEM((heads, tok_rows), F32),
            pltpu.VMEM((channels, model_width), BF16),
            pltpu.VMEM((tok_rows, model_width), BF16),
            pltpu.VMEM((1, channels), F32),
            pltpu.VMEM((1, model_width), F32),
            pltpu.VMEM((top_count, tok_rows), jnp.int32),
            pltpu.VMEM((1, tok_rows), F32),
            pltpu.VMEM((top_count, tok_rows), F32),
            sems((16,)),
            pltpu.VMEM((tok_rows, channels), F32),
            pltpu.VMEM((tok_rows, channels), BF16),
            pltpu.VMEM((heads, head_dim, 2 * head_dim), BF16),
            pltpu.VMEM((sp_count, share, head_dim, 2 * head_dim), BF16),
            pltpu.VMEM((sp_count, share, head_dim, 2 * head_dim), BF16),
            pltpu.VMEM((heads, head_dim, 2 * head_dim), BF16),
            pltpu.VMEM((tok_rows, channels), BF16),
            pltpu.VMEM((groups, tok_rows, cols), BF16),
            pltpu.VMEM((groups, tok_rows, cols), F32),
            pltpu.VMEM((groups, tok_rows, cols), BF16),
            pltpu.VMEM((groups, tok_rows, cols), BF16),
            pltpu.VMEM((groups, tok_rows, cols), BF16),
            pltpu.VMEM((tp_count, 8, tok_rows), F32),
            pltpu.VMEM((sp_count, per, cols), BF16),
            sems((sp_count,)),
            sems((sp_count,)),
            sems((sp_count,)),
            sems((sp_count,)),
            sems((groups,)),
            sems((groups,)),
            sems((groups,)),
            sems((groups,)),
            sems((tp_count,)),
            sems((tp_count,)),
            sems((sp_count,)),
            sems((sp_count,)),
            sems((tp_count, sp_count)),
            sems((tp_count, sp_count)),
            sems((tp_count, sp_count)),
            pltpu.VMEM((tok_rows, cols), F32),
            pltpu.VMEM((sp_count, per, model_width), BF16),
            pltpu.VMEM(specialist_switch_matrix.shape, BF16),
            pltpu.VMEM(specialist_expansion_matrix.shape, BF16),
            pltpu.VMEM(specialist_contraction_matrix.shape, BF16),
            pltpu.VMEM((sp_count, per, model_width), BF16),
            pltpu.VMEM((sp_count, groups, per, cols), BF16),
            pltpu.VMEM((sp_count, groups, per, cols), BF16),
            pltpu.VMEM((sp_count, groups, per, cols), BF16),
            pltpu.VMEM((sp_count, per, cols), BF16),
            pltpu.VMEM((sp_count, per, cols), BF16),
            sems((sp_count, groups)),
            sems((sp_count, groups)),
            sems((sp_count, groups)),
            sems((sp_count, groups)),
            sems((sp_count,)),
            sems((sp_count,)),
            sems((tp_count,)),
            sems((tp_count,)),
            sems((tp_count,)),
        ],
        compiler_params=pltpu.CompilerParams(
            collective_id=1, has_side_effects=True, vmem_limit_bytes=VMEM_LIMIT
        ),
    )(
        readout_query_vectors,
        attention_key_vectors,
        attention_content_vectors,
        step_size_preactivation,
        forgetting_preactivation,
        extra_forgetting_bias.T,
        blender_projection_matrix,
        skip_connection_stream,
        specialist_switch_matrix,
        specialist_expansion_matrix,
        specialist_contraction_matrix,
        subspace_normalizer_gain.reshape(1, channels),
        specialist_prenormal_gain.reshape(1, model_width),
        chosen_specialist_ids.T,
        cluster_router_chance.reshape(1, tok_rows),
        specialist_chance_within_cluster.T,
    )


def solution(mesh):
    in_specs = (
        P("sp", "tp"),
        P("sp", "tp"),
        P("sp", "tp"),
        P("sp", "tp"),
        P("sp", "tp"),
        P("sp", "tp"),
        P("tp"),
        P("sp", None),
        P("tp", None),
        P(),
        P("sp"),
        P("sp", None),
        P("sp", None),
        P("sp", None, "tp"),
        P("sp", None, "tp"),
        P("sp", "tp", None),
    )
    out_specs = P("sp", None)
    return jax.shard_map(body, mesh=mesh, in_specs=in_specs, out_specs=out_specs, check_vma=False)
```

```python
import functools
import math

import jax
import jax.numpy as jnp
from jax import lax
from jax.experimental import pallas as pl
from jax.experimental.pallas import tpu as pltpu
from jax.sharding import PartitionSpec as P

MESH = pl.DeviceIdType.MESH
F32 = jnp.float32
BF16 = jnp.bfloat16
VMEM_LIMIT = 48 * 1024 * 1024
SENDS = [6, 1, 5, 2, 3, 4, 7]
SCRIPT = [
    ("R", 1), ("R", 0), ("R", 6), ("R", 5), ("R", 2), ("R", 3), ("F", 5), ("F", 0), ("F", 2),
    ("R", 4), ("E", 2, 5), ("F", 3), ("M", 5), ("E", 3), ("F", 1), ("F", 4), ("R", 7), ("M", 3),
    ("F", 6), ("E", 4), ("E", 1), ("M", 4), ("T", 5), ("F", 7), ("M", 2), ("E", 7, 0), ("T", 3),
    ("E", 6), ("M", 7), ("T", 4), ("T", 7), ("M", 6), ("C", 3), ("M", 1), ("T", 2), ("T", 6),
    ("M", 0), ("T", 1), ("C", 2), ("T", 0), ("C", 5), ("C", 1), ("C", 0), ("C", 4), ("C", 7),
    ("C", 6),
]


def dot(left, right, axes=(1, 0)):
    return lax.dot_general(
        left, right, (((axes[0],), (axes[1],)), ((), ())), preferred_element_type=F32
    )


def halves(data):
    high = data.astype(BF16)
    return high, (data - high.astype(F32)).astype(BF16)


def stack(*parts):
    return jnp.concatenate(parts, axis=0)


def beside(*parts):
    return jnp.concatenate(parts, axis=1)


def mixer_setup(head_dim, segment, pairs):
    width = 2 * head_dim
    row = lax.broadcasted_iota(jnp.int32, (segment, width), 0)
    lane = lax.broadcasted_iota(jnp.int32, (segment, width), 1)
    col = lane & (segment - 1)
    return row, lane, col


def split_pair(head_dim):
    def pick(data):
        lane = lax.broadcasted_iota(jnp.int32, data.shape, 1)
        zero = jnp.zeros_like(data)
        return stack(jnp.where(lane < head_dim, data, zero), jnp.where(lane < head_dim, zero, data))

    return pick


def thirds(data):
    high = data.astype(BF16)
    rest = data - high.astype(F32)
    middle = rest.astype(BF16)
    return high, middle, (rest - middle.astype(F32)).astype(BF16)


def mixer_body(head_dim, segment, q_ref, k_ref, v_ref, a_ref, f_ref, b_ref, emit_map, between, emit_rows):
    rows, channels = q_ref.shape
    width = 2 * head_dim
    pairs = channels // width
    heads = channels // head_dim
    blocks = rows // segment
    shift = segment.bit_length() - 1
    row, lane, col = mixer_setup(head_dim, segment, pairs)
    strict, inclusive = row > col, row >= col
    bd = split_pair(head_dim)
    own = lax.broadcasted_iota(jnp.int32, (width, width), 0) // head_dim == (
        lax.broadcasted_iota(jnp.int32, (width, width), 1) // head_dim
    )
    ones = jnp.where(own, 1.0, 0.0).astype(BF16)
    ones = stack(ones, ones)
    spread = jnp.where(
        lax.rem(lax.broadcasted_iota(jnp.int32, (3 * heads, channels), 0), heads)
        == lax.broadcasted_iota(jnp.int32, (3 * heads, channels), 1) // head_dim,
        1.0,
        0.0,
    ).astype(BF16)
    pieces = stack(*[piece.astype(F32) for piece in thirds(b_ref[...])]).astype(BF16)
    bias = dot(pieces, spread, (0, 0))
    t0 = lax.broadcasted_iota(jnp.int32, (segment, segment), 0)
    t1 = lax.broadcasted_iota(jnp.int32, (segment, segment), 1)
    triangle = jnp.where(t0 >= t1, 1.0, 0.0).astype(BF16)
    triangle = beside(triangle, triangle, triangle)
    chains = [(p, b) for p in range(pairs) for b in range(blocks)]

    def prepare(p, b):
        at = (slice(b * segment, (b + 1) * segment), slice(p * width, (p + 1) * width))
        decay = -(0.6065306597126334 / (1.0 + jnp.exp(-f_ref[at]))) + bias[at]
        cumulative = dot(triangle, stack(*thirds(decay)))
        keys = k_ref[at].astype(F32)
        norms = dot(beside(*halves(keys * keys)), ones)
        removal = keys * lax.rsqrt(norms + 1e-06)
        beta = removal * (1.0 / (1.0 + jnp.exp(-a_ref[at].astype(F32))))
        closing = cumulative[segment - 1 :, :]
        grow = jnp.exp(-cumulative)
        fade = jnp.exp(closing - cumulative)
        c = {}
        c["alpha"] = -removal * jnp.exp(cumulative - decay)
        c["query"] = q_ref[at].astype(F32) * jnp.exp(cumulative)
        c["beta_hat"] = beta * grow
        c["key_hat"] = (keys * grow).astype(BF16)
        c["beta_bar"] = beta * fade
        c["key_bar"] = (keys * fade).astype(BF16)
        c["keep"] = jnp.where(row == col, jnp.exp(closing), 0.0)
        c["values"] = v_ref[at]
        return c

    C = [prepare(p, b) for p, b in chains]

    for c in C:
        ah, al = halves(c["alpha"])
        bh, bl = halves(c["beta_hat"])
        qh = c["query"].astype(BF16)
        by_beta = dot(stack(ah, al, qh), bd(bh), (1, 1))
        low = dot(ah, bd(bl), (1, 1))
        by_key = dot(stack(ah, qh), bd(c["key_hat"]), (1, 1))
        c["lower"] = jnp.where(strict, by_beta[:segment] + by_beta[segment : 2 * segment] + low, 0.0)
        c["read_remove"] = jnp.where(inclusive, by_beta[2 * segment :], 0.0).astype(BF16)
        c["remove_write"] = jnp.where(strict, by_key[:segment], 0.0)
        c["read_write"] = jnp.where(inclusive, by_key[segment:], 0.0).astype(BF16)
        c["ah"] = ah
        c["lh"], c["ll"] = halves(c["lower"])
    for c in C:
        wh, wl = halves(c["remove_write"])
        product = dot(stack(wh, wl, c["read_write"]), bd(c["values"]))
        c["side"] = product[:segment] + product[segment : 2 * segment]
        c["local"] = product[2 * segment :]
        c["inverse"] = jnp.where(
            row == col, 1.0, jnp.where((row >> 1) == (col >> 1), c["lower"], 0.0)
        )
    zero = jnp.zeros((segment, width), BF16)
    for s in range(1, shift):
        off = ((row >> (s + 1)) == (col >> (s + 1))) & ((row >> s) != (col >> s))
        for c in C:
            c["near"] = c["inverse"].astype(BF16)
            c["reach"] = dot(jnp.where(off, c["lh"], zero), bd(c["near"]))
        for c in C:
            c["inverse"] = c["inverse"] + dot(c["near"], bd(c["reach"].astype(BF16)))
    for c in C:
        c["near"] = c["inverse"].astype(BF16)
        c["both"] = beside(c["alpha"], c["side"])
        c["solved"] = dot(c["near"], beside(bd(c["ah"]), bd(c["side"].astype(BF16))))
    for c in C:
        sh, sl = halves(c["solved"])
        high = dot(stack(c["lh"], c["ll"]), beside(bd(sh[:, :width]), bd(sh[:, width:])))
        low = dot(c["lh"], beside(bd(sl[:, :width]), bd(sl[:, width:])))
        c["miss"] = c["both"] - c["solved"] + (high[:segment] + (high[segment:] + low))
    for c in C:
        miss = c["miss"].astype(BF16)
        c["solved"] = c["solved"] + dot(c["near"], beside(bd(miss[:, :width]), bd(miss[:, width:])))
    for c in C:
        sh, sl = halves(c["solved"])
        c["sh"] = sh
        bh, bl = halves(c["beta_bar"])
        left = stack(sh, sl, sh, beside(zero, c["values"]))
        step = dot(left, stack(bh, bh, bl, c["key_bar"]), (0, 0))
        first = lane < head_dim
        c["keep"] = c["keep"] + jnp.where(first, step[:head_dim], step[head_dim:width])
        c["add"] = jnp.where(first, step[width : width + head_dim], step[width + head_dim :])
    states = [[None] for _ in range(pairs)]
    now = [stack(C[p * blocks]["keep"], C[p * blocks]["add"]) for p in range(pairs)]
    for b in range(1, blocks):
        for p in range(pairs):
            c = C[p * blocks + b]
            kh, kl = halves(c["keep"])
            th, tl = halves(now[p])
            states[p].append(th)
            high = dot(stack(th, tl), bd(kh))
            low = dot(th, bd(kl))
            total = high[:width] + (high[width:] + low)
            now[p] = stack(total[:head_dim], total[head_dim:] + c["add"])
    for p in range(pairs):
        emit_map(p, now[p])
    between()
    for i, (p, b) in enumerate(chains):
        c = C[i]
        sh = c["sh"]
        read = dot(c["read_remove"], beside(bd(sh[:, :width]), bd(sh[:, width:])))
        c["read_map"] = c["query"] + read[:, :width]
        c["local"] = c["local"] + read[:, width:]
    for i, (p, b) in enumerate(chains):
        c = C[i]
        maps, local = c["read_map"].astype(BF16), c["local"]
        if b:
            th = states[p][b]
            seen = dot(maps, stack(bd(th[:head_dim]), bd(th[head_dim:])), (1, 1))
            maps, local = seen[:, :width].astype(BF16), local + seen[:, width:]
        emit_rows(p, b, maps, local)


def mate(me, d, count):
    total, bit = 0, 1
    while bit < count:
        own = lax.rem(lax.div(me, bit), 2)
        total = total + bit * (1 - own if d & bit else own)
        bit *= 2
    return total


def call_peers(sp_count, tp_count, sp, tp):
    barrier = pltpu.get_barrier_semaphore()
    for d in range(1, sp_count):
        pl.semaphore_signal(
            barrier, inc=1, device_id={"sp": lax.rem(sp + d, sp_count)}, device_id_type=MESH
        )
    for d in range(1, tp_count):
        pl.semaphore_signal(
            barrier, inc=1, device_id={"tp": lax.rem(tp + d, tp_count)}, device_id_type=MESH
        )


def meet_peers(sp_count, tp_count):
    pl.semaphore_wait(pltpu.get_barrier_semaphore(), sp_count + tp_count - 2)


def copy_to(src, dst, send, recv, device):
    return pltpu.make_async_remote_copy(
        src_ref=src,
        dst_ref=dst,
        send_sem=send,
        recv_sem=recv,
        device_id=device,
        device_id_type=MESH,
    )


def span(index, size):
    return pl.ds(pl.multiple_of(index * size, size), size)


def row_total(data, terms):
    ones = jnp.ones((8, data.shape[1]), BF16)
    total = None
    for _ in range(terms):
        piece = data.astype(BF16)
        data = data - piece.astype(F32)
        product = dot(ones, piece, (1, 1))
        total = product if total is None else total + product
    return total


def experts_back(
    sp_count, tp_count, ready, scale_of,
    rows_ref, switch_ref, expand_ref, contract_ref, hidden_ref, slots, weights,
    y_ref, from_sib, pair, from_peer, summed, back,
    s_sib, r_sib, s_peer, r_peer, s_back, r_back, ending,
):
    sp, tp = lax.axis_index("sp"), lax.axis_index("tp")
    per, model = y_ref.shape[1:]
    rows = hidden_ref.shape[0]
    cols = model // tp_count
    mine = span(tp, cols)
    groups = tp_count // 2
    core, group = lax.rem(tp, 2), lax.div(tp, 2)
    sibling = group * 2 + 1 - core
    others = [lax.rem(group + d, groups) for d in range(1, groups)]
    local = switch_ref.shape[0]
    capacity = per // local
    top = len(slots)
    places = lax.broadcasted_iota(jnp.int32, (rows, per), 1)

    def sib_copy(s, g):
        return copy_to(
            y_ref.at[s, :, span(g * 2 + 1 - core, cols)],
            from_sib.at[s, g],
            s_sib.at[s, g],
            r_sib.at[s, g],
            {"tp": sibling},
        )

    def peer_copy(s, g):
        return copy_to(
            pair.at[s, g],
            from_peer.at[s, group],
            s_peer.at[s, g],
            r_peer.at[s, group],
            {"tp": g * 2 + core},
        )

    def back_copy(t):
        return copy_to(summed.at[t], back.at[sp], s_back.at[t], r_back.at[sp], {"sp": t})

    def close(s, carry):
        sib_copy(s, group).wait_send()
        for g in others:
            sib_copy(s, g).wait_send()
            peer_copy(s, g).wait_send()
        return carry

    def sent(d, carry):
        back_copy(lax.rem(sp + d, sp_count)).wait_send()
        return carry

    ending.append(lambda: lax.fori_loop(0, sp_count, close, 0))
    ending.append(lambda: lax.fori_loop(1, sp_count, sent, 0))

    def expert(at, own):
        for s in at:
            ready(s)
        scales = [scale_of(s, o) for s, o in zip(at, own)]
        for e in range(local):
            inside = slice(e * capacity, (e + 1) * capacity)
            data = jnp.concatenate([rows_ref[s, inside, :] for s in at], axis=0)
            scale = jnp.concatenate([c[inside] for c in scales], axis=0)
            gate = dot(data, switch_ref[e]) * scale
            wide = dot(data, expand_ref[e]) * scale
            units = (gate / (1.0 + jnp.exp(-gate)) * wide).astype(BF16)
            value = dot(units, contract_ref[e]).astype(BF16)
            for c, s in enumerate(at):
                y_ref[s, inside, :] = value[c * capacity : (c + 1) * capacity]
        for s in at:
            for g in others:
                sib_copy(s, g).start()
            sib_copy(s, group).start()

    def meet(s):
        for g in others:
            sib_copy(s, g).wait_recv()
            pair[s, g] = (
                y_ref[s, :, span(g * 2 + core, cols)].astype(F32) + from_sib[s, g].astype(F32)
            ).astype(BF16)
            peer_copy(s, g).start()

    def total_up(s, own):
        sib_copy(s, group).wait_recv()
        total = y_ref[s, :, mine].astype(F32) + from_sib[s, group].astype(F32)
        for g in others:
            copy_to(
                from_peer.at[s, g],
                from_peer.at[s, g],
                s_peer.at[s, g],
                r_peer.at[s, g],
                {"tp": g * 2 + core},
            ).wait_recv()
            total = total + from_peer[s, g].astype(F32)
        if own:
            back[s] = total.astype(BF16)
        else:
            summed[s] = total.astype(BF16)
            back_copy(s).start()

    def combine(s, own):
        if not own:
            copy_to(back.at[s], back.at[s], s_back.at[s], r_back.at[s], {"sp": s}).wait_recv()
        chosen = [
            jnp.where(slots[k] == places + s * per, 1.0, 0.0).astype(BF16) for k in range(top)
        ]
        picked = dot(stack(*chosen), back[s])
        total = hidden_ref[...]
        for k in range(top):
            total = total + weights[k] * picked[k * rows : (k + 1) * rows]
        hidden_ref[...] = total

    return expert, meet, total_up, combine


def gather_out(tp_count, hidden_ref, out_ref, s_own, s_fwd, r_col):
    tp = lax.axis_index("tp")
    model = out_ref.shape[1]
    cols = model // tp_count
    mine = span(tp, cols)
    groups = tp_count // 2
    core, group = lax.rem(tp, 2), lax.div(tp, 2)
    sibling = group * 2 + 1 - core
    others = [lax.rem(group + d, groups) for d in range(1, groups)]
    out_ref[:, mine] = hidden_ref[...].astype(BF16)

    def own_copy(p):
        here = out_ref.at[:, mine]
        return copy_to(here, here, s_own.at[p], r_col.at[tp], {"tp": p})

    def forward(o):
        here = out_ref.at[:, span(o, cols)]
        return copy_to(here, here, s_fwd.at[o], r_col.at[o], {"tp": sibling})

    peers = [g * 2 + core for g in others]
    for p in peers:
        own_copy(p).start()
    own_copy(sibling).start()
    for p in peers:
        forward(p).wait_recv()
        forward(p).start()
    forward(sibling).wait_recv()
    for g in others:
        forward(g * 2 + 1 - core).wait_recv()
    own_copy(sibling).wait_send()
    for p in peers:
        own_copy(p).wait_send()
        forward(p).wait_send()


def plan(count, capacity):
    half = count // 2
    near, far = list(range(half)), list(range(half, count))
    if count == 8 and capacity == 128:
        return SENDS, SCRIPT
    chunk = max(1, 256 // capacity)
    steps = []
    for d in near + far:
        steps += [("R", d), ("F", d)]
    ranks = far + near[::-1]
    for i in range(0, count, chunk):
        steps.append(("E", *ranks[i : i + chunk]))
        steps += [("M", d) for d in ranks[i : i + chunk]]
        steps += [("T", d) for d in ranks[i : i + chunk]]
    return near[1:] + far, steps + [("C", d) for d in ranks]


def layer_kernel(
    head_dim, segment, sp_count, tp_count, experts, capacity,
    q_in, k_in, v_in, a_in, f_in, b_in, w_in, skip_in, switch_in, expand_in, contract_in,
    norm_in, gain_in, ids_in, chance_in, within_in,
    out_ref,
    q_ref, k_ref, v_ref, a_ref, f_ref, b_ref, w_ref, skip_ref,
    norm_ref, gain_ref, ids_ref, chance_ref, within_ref, s_in,
    local, maps_in, ka, got, fold, st, mixed,
    lent, kept, from_sib, pair, from_peer, squares, outgoing,
    s_map, r_map, s_fold, r_fold, s_sib, r_sib, s_peer, r_peer,
    s_sq, r_sq, s_out, r_out, s_own, s_fwd, r_col,
    hidden_ref, rows_ref, switch_ref, expand_ref, contract_ref,
    scale_out, scale_in, s_scale, r_scale, *back_refs,
):
    sp, tp = lax.axis_index("sp"), lax.axis_index("tp")
    rows, channels = q_in.shape
    model = skip_in.shape[1]
    cols = model // tp_count
    width = 2 * head_dim
    heads = channels // head_dim
    share = max(1, heads // sp_count)
    workers = heads // share
    mine = span(tp, cols)
    groups = tp_count // 2
    core, group = lax.rem(tp, 2), lax.div(tp, 2)
    sibling = group * 2 + 1 - core
    others = [lax.rem(group + g, groups) for g in range(1, groups)]
    early = [
        pltpu.make_async_copy(src, dst, s_in.at[i])
        for i, (src, dst) in enumerate(
            [(f_in, f_ref), (b_in, b_ref), (k_in, k_ref), (a_in, a_ref), (q_in, q_ref),
             (v_in, v_ref), (norm_in, norm_ref), (gain_in, gain_ref), (ids_in, ids_ref),
             (chance_in, chance_ref), (within_in, within_ref), (w_in, w_ref),
             (skip_in, skip_ref), (switch_in, switch_ref), (expand_in, expand_ref),
             (contract_in, contract_ref)]
        )
    ]
    for copy in early[:6]:
        copy.start()
    call_peers(sp_count, tp_count, sp, tp)
    for copy in early[:6]:
        copy.wait()
    for copy in early[6:]:
        copy.start()
    ending = []

    def unless_me(t, action):
        pl.when(t != sp)(action)

    def map_copy(t, owner):
        return copy_to(
            ka.at[pl.ds(t * share, share)], got.at[owner], s_map.at[t], r_map.at[owner], {"sp": t}
        )

    def fold_copy(t, owner):
        return copy_to(
            fold.at[t], st.at[pl.ds(owner * share, share)], s_fold.at[t], r_fold.at[owner], {"sp": t}
        )

    def emit_map(p, state):
        for h in range(2):
            part = slice(h * head_dim, (h + 1) * head_dim)
            ka[2 * p + h] = beside(state[:head_dim, part], state[head_dim:, part]).astype(BF16)

    def send_maps():
        meet_peers(sp_count, tp_count)
        if workers == sp_count:
            for d in range(1, sp_count):
                map_copy(mate(sp, d, sp_count), sp).start()
        else:
            for t in range(workers):
                unless_me(t, lambda t=t: map_copy(t, sp).start())

    def emit_rows(p, b, maps, out):
        at = (slice(b * segment, (b + 1) * segment), slice(p * width, (p + 1) * width))
        local[at] = out
        maps_in[at] = maps

    mixer_body(
        head_dim, segment, q_ref, k_ref, v_ref, a_ref, f_ref, b_ref, emit_map, send_maps, emit_rows
    )

    for copy in early[6:]:
        copy.wait()
    top = ids_ref.shape[0]
    within = within_ref[...]
    shares = chance_ref[...] * within / jnp.sum(within, axis=0, keepdims=True)
    lines = [ids_ref[k : k + 1, :].astype(F32) for k in range(top)]
    lines = lines + [shares[k : k + 1, :] for k in range(top)]
    place = lax.broadcasted_iota(jnp.int32, (8, rows), 0)
    table = jnp.zeros((8, rows), F32)
    for k in range(2 * top):
        table = jnp.where(place == k, lines[k], table)
    pieces = stack(*[piece.astype(F32) for piece in thirds(table)]).astype(BF16)
    unit = jnp.where(
        lax.rem(lax.broadcasted_iota(jnp.int32, (24, 128), 0), 8)
        == lax.broadcasted_iota(jnp.int32, (24, 128), 1),
        1.0,
        0.0,
    ).astype(BF16)
    upright = dot(pieces, unit, (0, 0))
    weights = [upright[:, top + k : top + k + 1] for k in range(top)]
    lanes = lax.broadcasted_iota(jnp.int32, (rows, experts), 1).astype(F32)
    named = [upright[:, k : k + 1] == lanes for k in range(top)]
    anyone = sum(jnp.where(n, 1.0, 0.0) for n in named).astype(BF16)
    r0 = lax.broadcasted_iota(jnp.int32, (rows, rows), 0)
    r1 = lax.broadcasted_iota(jnp.int32, (rows, rows), 1)
    before = dot(jnp.where(r0 > r1, 1.0, 0.0).astype(BF16), anyone)
    slots = [
        jnp.sum(
            jnp.where(n, before + lanes * capacity, 0.0), axis=1, keepdims=True
        ).astype(jnp.int32)
        for n in named
    ]
    def chain():
        got[sp] = ka[pl.ds(sp * share, share)]
        half = lax.div(lax.broadcasted_iota(jnp.int32, (head_dim, width), 1), head_dim)
        places = [half == lax.rem(sp * share + i, 2) for i in range(share)]
        state = [jnp.zeros((head_dim, head_dim), F32) for _ in range(share)]
        for j in range(sp_count):
            unless_me(
                j,
                lambda j=j: copy_to(
                    got.at[j], got.at[j], s_map.at[0], r_map.at[j], {"sp": j}
                ).wait_recv(),
            )
            for i in range(share):
                fold[j, i] = jnp.where(places[i], beside(state[i], state[i]), 0.0).astype(BF16)
            unless_me(j, lambda j=j: fold_copy(j, sp).start())
            for i in range(share):
                both = got[j, i]
                product = dot(stack(*halves(state[i])), both[:, :head_dim])
                state[i] = product[:head_dim] + product[head_dim:] + both[:, head_dim:].astype(F32)
        st[pl.ds(sp * share, share)] = fold[sp]

    def map_sent():
        for t in range(workers):
            unless_me(t, lambda t=t: map_copy(t, sp).wait_send())

    def fold_sent():
        for t in range(sp_count):
            unless_me(t, lambda t=t: fold_copy(t, sp).wait_send())

    ending.append(map_sent)
    ending.append(fold_sent if workers == sp_count else lambda: pl.when(sp < workers)(fold_sent))
    if workers == sp_count:
        chain()
    else:
        pl.when(sp < workers)(chain)
    ones = jnp.where(
        lax.div(lax.broadcasted_iota(jnp.int32, (width, width), 0), head_dim)
        == lax.div(lax.broadcasted_iota(jnp.int32, (width, width), 1), head_dim),
        1.0 / head_dim,
        0.0,
    ).astype(BF16)
    ones = stack(ones, ones)
    for t in range(workers):
        unless_me(
            t,
            lambda t=t: copy_to(
                fold.at[t], st.at[pl.ds(t * share, share)], s_fold.at[0], r_fold.at[t], {"sp": t}
            ).wait_recv(),
        )
    for p in range(heads // 2):
        part = slice(p * width, (p + 1) * width)
        states = stack(st[2 * p], st[2 * p + 1])
        output = local[:, part] + dot(maps_in[:, part], states, (1, 1))
        centered = output - dot(beside(*halves(output)), ones)
        spread = dot(beside(*halves(centered * centered)), ones)
        mixed[:, part] = (centered * lax.rsqrt(spread + 0.00064) * norm_ref[:, part]).astype(BF16)

    def sib_copy(g):
        return copy_to(lent.at[g], from_sib.at[g], s_sib.at[g], r_sib.at[g], {"tp": sibling})

    def peer_copy(g):
        return copy_to(
            pair.at[g], from_peer.at[group], s_peer.at[g], r_peer.at[group], {"tp": g * 2 + core}
        )

    ending.append(lambda: [sib_copy(g).wait_send() for g in others + [group]])
    ending.append(lambda: [peer_copy(g).wait_send() for g in others])
    for g in others + [group]:
        lent[g] = dot(mixed[...], w_ref[:, span(g * 2 + 1 - core, cols)]).astype(BF16)
        sib_copy(g).start()
    for g in others + [group]:
        kept[g] = dot(mixed[...], w_ref[:, span(g * 2 + core, cols)])
    for g in others:
        sib_copy(g).wait_recv()
        pair[g] = (kept[g] + from_sib[g].astype(F32)).astype(BF16)
        peer_copy(g).start()
    sib_copy(group).wait_recv()
    hidden = skip_ref[:, mine].astype(F32) + (kept[group] + from_sib[group].astype(F32))
    for g in others:
        copy_to(
            pair.at[g], from_peer.at[g], s_peer.at[g], r_peer.at[g], {"tp": g * 2 + core}
        ).wait_recv()
        hidden = hidden + from_peer[g].astype(F32)
    hidden_ref[...] = hidden
    squares[tp] = row_total(hidden * hidden, 3)

    def square_copy(p):
        return copy_to(squares.at[tp], squares.at[tp], s_sq.at[p], r_sq.at[tp], {"tp": p})

    ending.append(
        lambda: [square_copy(lax.rem(tp + d, tp_count)).wait_send() for d in range(1, tp_count)]
    )
    for d in range(1, tp_count):
        square_copy(lax.rem(tp + d, tp_count)).start()
    normed = (hidden * gain_ref[:, mine]).astype(BF16)

    per = experts // sp_count * capacity
    places = lax.broadcasted_iota(jnp.int32, (rows, per), 1)

    def chosen_for(t):
        at = places + t * per
        chosen = slots[0] == at
        for s in slots[1:]:
            chosen = chosen | (s == at)
        return jnp.where(chosen, 1.0, 0.0).astype(BF16)

    def block_for(t):
        return dot(chosen_for(t), normed, (0, 0)).astype(BF16)

    def out_copy(t):
        return copy_to(
            outgoing.at[t], rows_ref.at[sp, :, mine], s_out.at[t], r_out.at[sp], {"sp": t}
        )

    def own_copy(p, s):
        here = rows_ref.at[s, :, mine]
        return copy_to(here, here, s_own.at[p, s], r_col.at[tp, s], {"tp": p})

    def forward(o, s):
        here = rows_ref.at[s, :, span(o, cols)]
        return copy_to(here, here, s_fwd.at[o, s], r_col.at[o, s], {"tp": sibling})

    peers = [g * 2 + core for g in others]

    def pass_on(s):
        for p in peers:
            own_copy(p, s).start()
        own_copy(sibling, s).start()

    def settle(s, carry):
        own_copy(sibling, s).wait_send()
        for p in peers:
            own_copy(p, s).wait_send()
            forward(p, s).wait_send()
        return carry

    def sent(d, carry):
        out_copy(lax.rem(sp + d, sp_count)).wait_send()
        return carry

    ending.append(lambda: lax.fori_loop(0, sp_count, settle, 0))
    ending.append(lambda: lax.fori_loop(1, sp_count, sent, 0))
    def ready(s):
        forward(sibling, s).wait_recv()
        for g in others:
            forward(g * 2 + 1 - core, s).wait_recv()

    sends, steps = plan(sp_count, capacity)

    def source(d):
        return mate(sp, d, sp_count)

    y_ref, sib_back, pair_back, peer_back, summed, returned = back_refs[:6]
    s_sib2, r_sib2, s_peer2, r_peer2, s_back, r_back, s_last, s_fwd2, r_last = back_refs[6:]
    for d in sends:
        t = mate(sp, d, sp_count)
        outgoing[t] = block_for(t)
        out_copy(t).start()
    rows_ref[sp, :, mine] = block_for(sp)
    total = squares[tp]
    for d in range(1, tp_count):
        p = lax.rem(tp + d, tp_count)
        copy_to(squares.at[p], squares.at[p], s_sq.at[p], r_sq.at[p], {"tp": p}).wait_recv()
        total = total + squares[p]
    inverse = [piece.astype(F32) for piece in thirds(lax.rsqrt(total / model + 1e-06))]
    inverse = stack(*inverse).astype(BF16)

    def scale_for(t):
        product = dot(inverse, chosen_for(t))
        return product[:8] + product[8:16] + product[16:]

    def scale_copy(t):
        return copy_to(
            scale_out.at[t], scale_in.at[sp], s_scale.at[t], r_scale.at[sp], {"sp": t}
        )

    def scale_sent(d, carry):
        scale_copy(lax.rem(sp + d, sp_count)).wait_send()
        return carry

    ending.append(lambda: lax.fori_loop(1, sp_count, scale_sent, 0))
    for d in sends:
        t = mate(sp, d, sp_count)
        scale_out[t] = scale_for(t)
        scale_copy(t).start()
    scale_in[sp] = scale_for(sp)
    one = jnp.where(
        lax.rem(lax.broadcasted_iota(jnp.int32, (24, 128), 0), 8) == 0, 1.0, 0.0
    ).astype(BF16)

    def scale_of(s, own):
        if not own:
            copy_to(
                scale_in.at[s], scale_in.at[s], s_scale.at[s], r_scale.at[s], {"sp": s}
            ).wait_recv()
        pieces = stack(*[piece.astype(F32) for piece in thirds(scale_in[s])]).astype(BF16)
        return dot(pieces, one, (0, 0))[:, :1]

    expert, meet, total_up, combine = experts_back(
        sp_count, tp_count, ready, scale_of,
        rows_ref, switch_ref, expand_ref, contract_ref, hidden_ref, slots, weights,
        y_ref, sib_back, pair_back, peer_back, summed, returned,
        s_sib2, r_sib2, s_peer2, r_peer2, s_back, r_back, ending,
    )
    for kind, *which in steps:
        for d in which[:1] if kind == "E" else which:
            s = source(d)
            if kind == "R":
                if d:
                    here = rows_ref.at[s, :, mine]
                    copy_to(here, here, s_out.at[s], r_out.at[s], {"sp": s}).wait_recv()
                pass_on(s)
            if kind == "F":
                for o in peers:
                    forward(o, s).wait_recv()
                    forward(o, s).start()
            if kind == "E":
                expert([source(i) for i in which], [i == 0 for i in which])
            if kind == "M":
                meet(s)
            if kind == "T":
                total_up(s, d == 0)
            if kind == "C":
                combine(s, d == 0)
    gather_out(tp_count, hidden_ref, out_ref, s_last, s_fwd2, r_last)
    for wait in ending:
        wait()


def body(
    readout_query_vectors,
    attention_key_vectors,
    attention_content_vectors,
    step_size_preactivation,
    forgetting_preactivation,
    extra_forgetting_bias,
    subspace_normalizer_gain,
    skip_connection_stream,
    blender_projection_matrix,
    specialist_prenormal_gain,
    cluster_router_chance,
    specialist_chance_within_cluster,
    chosen_specialist_ids,
    specialist_switch_matrix,
    specialist_expansion_matrix,
    specialist_contraction_matrix,
):
    tok_rows, model_width = skip_connection_stream.shape
    sp_count, tp_count = lax.axis_size("sp"), lax.axis_size("tp")
    local_experts = specialist_switch_matrix.shape[0]
    experts = local_experts * sp_count
    top_count = chosen_specialist_ids.shape[1]
    capacity = 2 * tok_rows * top_count // experts
    cols = model_width // tp_count
    per = local_experts * capacity
    groups = tp_count // 2
    channels = readout_query_vectors.shape[1]
    heads = extra_forgetting_bias.shape[1]
    head_dim = channels // heads
    share = max(1, heads // sp_count)
    vmem = pl.BlockSpec(memory_space=pltpu.VMEM)
    hbm = pl.BlockSpec(memory_space=pltpu.HBM)
    sems = pltpu.SemaphoreType.DMA
    return pl.pallas_call(
        functools.partial(
            layer_kernel, head_dim, min(64, tok_rows), sp_count, tp_count, experts, capacity
        ),
        out_shape=jax.ShapeDtypeStruct((tok_rows, model_width), BF16),
        in_specs=[hbm] * 16,
        out_specs=vmem,
        scratch_shapes=[
            pltpu.VMEM((tok_rows, channels), BF16),
            pltpu.VMEM((tok_rows, channels), BF16),
            pltpu.VMEM((tok_rows, channels), BF16),
            pltpu.VMEM((tok_rows, channels), BF16),
            pltpu.VMEM((tok_rows, channels), F32),
            pltpu.VMEM((heads, tok_rows), F32),
            pltpu.VMEM((channels, model_width), BF16),
            pltpu.VMEM((tok_rows, model_width), BF16),
            pltpu.VMEM((1, channels), F32),
            pltpu.VMEM((1, model_width), F32),
            pltpu.VMEM((top_count, tok_rows), jnp.int32),
            pltpu.VMEM((1, tok_rows), F32),
            pltpu.VMEM((top_count, tok_rows), F32),
            sems((16,)),
            pltpu.VMEM((tok_rows, channels), F32),
            pltpu.VMEM((tok_rows, channels), BF16),
            pltpu.VMEM((heads, head_dim, 2 * head_dim), BF16),
            pltpu.VMEM((sp_count, share, head_dim, 2 * head_dim), BF16),
            pltpu.VMEM((sp_count, share, head_dim, 2 * head_dim), BF16),
            pltpu.VMEM((heads, head_dim, 2 * head_dim), BF16),
            pltpu.VMEM((tok_rows, channels), BF16),
            pltpu.VMEM((groups, tok_rows, cols), BF16),
            pltpu.VMEM((groups, tok_rows, cols), F32),
            pltpu.VMEM((groups, tok_rows, cols), BF16),
            pltpu.VMEM((groups, tok_rows, cols), BF16),
            pltpu.VMEM((groups, tok_rows, cols), BF16),
            pltpu.VMEM((tp_count, 8, tok_rows), F32),
            pltpu.VMEM((sp_count, per, cols), BF16),
            sems((sp_count,)),
            sems((sp_count,)),
            sems((sp_count,)),
            sems((sp_count,)),
            sems((groups,)),
            sems((groups,)),
            sems((groups,)),
            sems((groups,)),
            sems((tp_count,)),
            sems((tp_count,)),
            sems((sp_count,)),
            sems((sp_count,)),
            sems((tp_count, sp_count)),
            sems((tp_count, sp_count)),
            sems((tp_count, sp_count)),
            pltpu.VMEM((tok_rows, cols), F32),
            pltpu.VMEM((sp_count, per, model_width), BF16),
            pltpu.VMEM(specialist_switch_matrix.shape, BF16),
            pltpu.VMEM(specialist_expansion_matrix.shape, BF16),
            pltpu.VMEM(specialist_contraction_matrix.shape, BF16),
            pltpu.VMEM((sp_count, 8, per), F32),
            pltpu.VMEM((sp_count, 8, per), F32),
            sems((sp_count,)),
            sems((sp_count,)),
            pltpu.VMEM((sp_count, per, model_width), BF16),
            pltpu.VMEM((sp_count, groups, per, cols), BF16),
            pltpu.VMEM((sp_count, groups, per, cols), BF16),
            pltpu.VMEM((sp_count, groups, per, cols), BF16),
            pltpu.VMEM((sp_count, per, cols), BF16),
            pltpu.VMEM((sp_count, per, cols), BF16),
            sems((sp_count, groups)),
            sems((sp_count, groups)),
            sems((sp_count, groups)),
            sems((sp_count, groups)),
            sems((sp_count,)),
            sems((sp_count,)),
            sems((tp_count,)),
            sems((tp_count,)),
            sems((tp_count,)),
        ],
        compiler_params=pltpu.CompilerParams(
            collective_id=1, has_side_effects=True, vmem_limit_bytes=VMEM_LIMIT
        ),
    )(
        *[
            pltpu.with_memory_space_constraint(operand, pltpu.HBM)
            for operand in (
                readout_query_vectors,
                attention_key_vectors,
                attention_content_vectors,
                step_size_preactivation,
                forgetting_preactivation,
                extra_forgetting_bias.T,
                blender_projection_matrix,
                skip_connection_stream,
                specialist_switch_matrix,
                specialist_expansion_matrix,
                specialist_contraction_matrix,
                subspace_normalizer_gain.reshape(1, channels),
                specialist_prenormal_gain.reshape(1, model_width),
                chosen_specialist_ids.T,
                cluster_router_chance.reshape(1, tok_rows),
                specialist_chance_within_cluster.T,
            )
        ]
    )


def solution(mesh):
    in_specs = (
        P("sp", "tp"),
        P("sp", "tp"),
        P("sp", "tp"),
        P("sp", "tp"),
        P("sp", "tp"),
        P("sp", "tp"),
        P("tp"),
        P("sp", None),
        P("tp", None),
        P(),
        P("sp"),
        P("sp", None),
        P("sp", None),
        P("sp", None, "tp"),
        P("sp", None, "tp"),
        P("sp", "tp", None),
    )
    out_specs = P("sp", None)
    return jax.shard_map(body, mesh=mesh, in_specs=in_specs, out_specs=out_specs, check_vma=False)
```

```python
import functools
import math

import jax
import jax.numpy as jnp
from jax import lax
from jax.experimental import pallas as pl
from jax.experimental.pallas import tpu as pltpu
from jax.sharding import PartitionSpec as P

MESH = pl.DeviceIdType.MESH
F32 = jnp.float32
BF16 = jnp.bfloat16
VMEM_LIMIT = 48 * 1024 * 1024
SENDS = [6, 1, 5, 2, 3, 4, 7]
SCRIPT = [
    ("R", 1), ("R", 0), ("R", 6), ("R", 5), ("R", 2), ("R", 3), ("F", 5), ("F", 0), ("F", 2),
    ("R", 4), ("E", 2, 5), ("F", 3), ("M", 5), ("E", 3), ("F", 1), ("F", 4), ("R", 7), ("M", 3),
    ("F", 6), ("E", 4), ("E", 1), ("M", 4), ("T", 5), ("F", 7), ("M", 2), ("E", 7, 0), ("T", 3),
    ("E", 6), ("M", 7), ("T", 4), ("T", 7), ("M", 6), ("C", 3), ("M", 1), ("T", 2), ("T", 6),
    ("M", 0), ("T", 1), ("C", 2), ("T", 0), ("C", 5), ("C", 1), ("C", 0), ("C", 4), ("C", 7),
    ("C", 6),
]


def dot(left, right, axes=(1, 0)):
    return lax.dot_general(
        left, right, (((axes[0],), (axes[1],)), ((), ())), preferred_element_type=F32
    )


def halves(data):
    high = data.astype(BF16)
    return high, (data - high.astype(F32)).astype(BF16)


def stack(*parts):
    return jnp.concatenate(parts, axis=0)


def beside(*parts):
    return jnp.concatenate(parts, axis=1)


def mixer_setup(head_dim, segment, pairs):
    width = 2 * head_dim
    row = lax.broadcasted_iota(jnp.int32, (segment, width), 0)
    lane = lax.broadcasted_iota(jnp.int32, (segment, width), 1)
    col = lane & (segment - 1)
    return row, lane, col


def split_pair(head_dim):
    def pick(data):
        lane = lax.broadcasted_iota(jnp.int32, data.shape, 1)
        zero = jnp.zeros_like(data)
        return stack(jnp.where(lane < head_dim, data, zero), jnp.where(lane < head_dim, zero, data))

    return pick


def thirds(data):
    high = data.astype(BF16)
    rest = data - high.astype(F32)
    middle = rest.astype(BF16)
    return high, middle, (rest - middle.astype(F32)).astype(BF16)


def mixer_body(head_dim, segment, q_ref, k_ref, v_ref, a_ref, f_ref, b_ref, emit_map, between, emit_rows):
    rows, channels = q_ref.shape
    width = 2 * head_dim
    pairs = channels // width
    heads = channels // head_dim
    blocks = rows // segment
    shift = segment.bit_length() - 1
    row, lane, col = mixer_setup(head_dim, segment, pairs)
    strict, inclusive = row > col, row >= col
    bd = split_pair(head_dim)
    own = lax.broadcasted_iota(jnp.int32, (width, width), 0) // head_dim == (
        lax.broadcasted_iota(jnp.int32, (width, width), 1) // head_dim
    )
    ones = jnp.where(own, 1.0, 0.0).astype(BF16)
    ones = stack(ones, ones)
    spread = jnp.where(
        lax.rem(lax.broadcasted_iota(jnp.int32, (3 * heads, channels), 0), heads)
        == lax.broadcasted_iota(jnp.int32, (3 * heads, channels), 1) // head_dim,
        1.0,
        0.0,
    ).astype(BF16)
    pieces = stack(*[piece.astype(F32) for piece in thirds(b_ref[...])]).astype(BF16)
    bias = dot(pieces, spread, (0, 0))
    t0 = lax.broadcasted_iota(jnp.int32, (segment, segment), 0)
    t1 = lax.broadcasted_iota(jnp.int32, (segment, segment), 1)
    triangle = jnp.where(t0 >= t1, 1.0, 0.0).astype(BF16)
    triangle = beside(triangle, triangle, triangle)
    chains = [(p, b) for p in range(pairs) for b in range(blocks)]

    def prepare(p, b):
        at = (slice(b * segment, (b + 1) * segment), slice(p * width, (p + 1) * width))
        decay = -(0.6065306597126334 / (1.0 + jnp.exp(-f_ref[at]))) + bias[at]
        cumulative = dot(triangle, stack(*thirds(decay)))
        keys = k_ref[at].astype(F32)
        norms = dot(beside(*halves(keys * keys)), ones)
        removal = keys * lax.rsqrt(norms + 1e-06)
        beta = removal * (1.0 / (1.0 + jnp.exp(-a_ref[at].astype(F32))))
        closing = cumulative[segment - 1 :, :]
        grow = jnp.exp(-cumulative)
        fade = jnp.exp(closing - cumulative)
        c = {}
        c["alpha"] = -removal * jnp.exp(cumulative - decay)
        c["query"] = q_ref[at].astype(F32) * jnp.exp(cumulative)
        c["beta_hat"] = beta * grow
        c["key_hat"] = (keys * grow).astype(BF16)
        c["beta_bar"] = beta * fade
        c["key_bar"] = (keys * fade).astype(BF16)
        c["keep"] = jnp.where(row == col, jnp.exp(closing), 0.0)
        c["values"] = v_ref[at]
        return c

    C = [prepare(p, b) for p, b in chains]

    for c in C:
        ah, al = halves(c["alpha"])
        bh, bl = halves(c["beta_hat"])
        qh = c["query"].astype(BF16)
        by_beta = dot(stack(ah, al, qh), bd(bh), (1, 1))
        low = dot(ah, bd(bl), (1, 1))
        by_key = dot(stack(ah, qh), bd(c["key_hat"]), (1, 1))
        c["lower"] = jnp.where(strict, by_beta[:segment] + by_beta[segment : 2 * segment] + low, 0.0)
        c["read_remove"] = jnp.where(inclusive, by_beta[2 * segment :], 0.0).astype(BF16)
        c["remove_write"] = jnp.where(strict, by_key[:segment], 0.0)
        c["read_write"] = jnp.where(inclusive, by_key[segment:], 0.0).astype(BF16)
        c["ah"] = ah
        c["lh"], c["ll"] = halves(c["lower"])
    for c in C:
        wh, wl = halves(c["remove_write"])
        product = dot(stack(wh, wl, c["read_write"]), bd(c["values"]))
        c["side"] = product[:segment] + product[segment : 2 * segment]
        c["local"] = product[2 * segment :]
        c["inverse"] = jnp.where(
            row == col, 1.0, jnp.where((row >> 1) == (col >> 1), c["lower"], 0.0)
        )
    zero = jnp.zeros((segment, width), BF16)
    for s in range(1, shift):
        off = ((row >> (s + 1)) == (col >> (s + 1))) & ((row >> s) != (col >> s))
        for c in C:
            c["near"] = c["inverse"].astype(BF16)
            c["reach"] = dot(jnp.where(off, c["lh"], zero), bd(c["near"]))
        for c in C:
            c["inverse"] = c["inverse"] + dot(c["near"], bd(c["reach"].astype(BF16)))
    for c in C:
        c["near"] = c["inverse"].astype(BF16)
        c["both"] = beside(c["alpha"], c["side"])
        c["solved"] = dot(c["near"], beside(bd(c["ah"]), bd(c["side"].astype(BF16))))
    for c in C:
        sh, sl = halves(c["solved"])
        high = dot(stack(c["lh"], c["ll"]), beside(bd(sh[:, :width]), bd(sh[:, width:])))
        low = dot(c["lh"], beside(bd(sl[:, :width]), bd(sl[:, width:])))
        c["miss"] = c["both"] - c["solved"] + (high[:segment] + (high[segment:] + low))
    for c in C:
        miss = c["miss"].astype(BF16)
        c["solved"] = c["solved"] + dot(c["near"], beside(bd(miss[:, :width]), bd(miss[:, width:])))
    for c in C:
        sh, sl = halves(c["solved"])
        c["sh"] = sh
        bh, bl = halves(c["beta_bar"])
        left = stack(sh, sl, sh, beside(zero, c["values"]))
        step = dot(left, stack(bh, bh, bl, c["key_bar"]), (0, 0))
        first = lane < head_dim
        c["keep"] = c["keep"] + jnp.where(first, step[:head_dim], step[head_dim:width])
        c["add"] = jnp.where(first, step[width : width + head_dim], step[width + head_dim :])
    states = [[None] for _ in range(pairs)]
    now = [stack(C[p * blocks]["keep"], C[p * blocks]["add"]) for p in range(pairs)]
    for b in range(1, blocks):
        for p in range(pairs):
            c = C[p * blocks + b]
            kh, kl = halves(c["keep"])
            th, tl = halves(now[p])
            states[p].append(th)
            high = dot(stack(th, tl), bd(kh))
            low = dot(th, bd(kl))
            total = high[:width] + (high[width:] + low)
            now[p] = stack(total[:head_dim], total[head_dim:] + c["add"])
    for p in range(pairs):
        emit_map(p, now[p])
    between()
    for i, (p, b) in enumerate(chains):
        c = C[i]
        sh = c["sh"]
        read = dot(c["read_remove"], beside(bd(sh[:, :width]), bd(sh[:, width:])))
        c["read_map"] = c["query"] + read[:, :width]
        c["local"] = c["local"] + read[:, width:]
    for i, (p, b) in enumerate(chains):
        c = C[i]
        maps, local = c["read_map"].astype(BF16), c["local"]
        if b:
            th = states[p][b]
            seen = dot(maps, stack(bd(th[:head_dim]), bd(th[head_dim:])), (1, 1))
            maps, local = seen[:, :width].astype(BF16), local + seen[:, width:]
        emit_rows(p, b, maps, local)


def mate(me, d, count):
    total, bit = 0, 1
    while bit < count:
        own = lax.rem(lax.div(me, bit), 2)
        total = total + bit * (1 - own if d & bit else own)
        bit *= 2
    return total


def call_peers(sp_count, tp_count, sp, tp):
    barrier = pltpu.get_barrier_semaphore()
    for d in range(1, sp_count):
        pl.semaphore_signal(
            barrier, inc=1, device_id={"sp": lax.rem(sp + d, sp_count)}, device_id_type=MESH
        )
    for d in range(1, tp_count):
        pl.semaphore_signal(
            barrier, inc=1, device_id={"tp": lax.rem(tp + d, tp_count)}, device_id_type=MESH
        )


def meet_peers(sp_count, tp_count):
    pl.semaphore_wait(pltpu.get_barrier_semaphore(), sp_count + tp_count - 2)


def cuts_of(rows):
    size = rows // 2 if rows >= 128 else rows
    return [(h, slice(h * size, (h + 1) * size)) for h in range(rows // size)]


def copy_to(src, dst, send, recv, device):
    return pltpu.make_async_remote_copy(
        src_ref=src,
        dst_ref=dst,
        send_sem=send,
        recv_sem=recv,
        device_id=device,
        device_id_type=MESH,
    )


def span(index, size):
    return pl.ds(pl.multiple_of(index * size, size), size)


def row_total(data, terms):
    ones = jnp.ones((8, data.shape[1]), BF16)
    total = None
    for _ in range(terms):
        piece = data.astype(BF16)
        data = data - piece.astype(F32)
        product = dot(ones, piece, (1, 1))
        total = product if total is None else total + product
    return total


def experts_back(
    sp_count, tp_count, ready, scale_of,
    rows_ref, switch_ref, expand_ref, contract_ref, hidden_ref, slots, weights,
    y_ref, from_sib, pair, from_peer, summed, back,
    s_sib, r_sib, s_peer, r_peer, s_back, r_back, ending,
):
    sp, tp = lax.axis_index("sp"), lax.axis_index("tp")
    per, model = y_ref.shape[1:]
    rows = hidden_ref.shape[0]
    cols = model // tp_count
    mine = span(tp, cols)
    groups = tp_count // 2
    core, group = lax.rem(tp, 2), lax.div(tp, 2)
    sibling = group * 2 + 1 - core
    others = [lax.rem(group + d, groups) for d in range(1, groups)]
    local = switch_ref.shape[0]
    capacity = per // local
    top = len(slots)
    places = lax.broadcasted_iota(jnp.int32, (rows, per), 1)

    def sib_copy(s, g):
        return copy_to(
            y_ref.at[s, :, span(g * 2 + 1 - core, cols)],
            from_sib.at[s, g],
            s_sib.at[s, g],
            r_sib.at[s, g],
            {"tp": sibling},
        )

    cuts = cuts_of(per)

    def peer_copy(s, g, h, at):
        return copy_to(
            pair.at[s, g, at],
            from_peer.at[s, group, at],
            s_peer.at[s, g, h],
            r_peer.at[s, group, h],
            {"tp": g * 2 + core},
        )

    def back_copy(t, h, at):
        return copy_to(
            summed.at[t, at], back.at[sp, at], s_back.at[t, h], r_back.at[sp, h], {"sp": t}
        )

    def close(s, carry):
        sib_copy(s, group).wait_send()
        for g in others:
            sib_copy(s, g).wait_send()
            for cut in cuts:
                peer_copy(s, g, *cut).wait_send()
        return carry

    def sent(d, carry):
        for cut in cuts:
            back_copy(lax.rem(sp + d, sp_count), *cut).wait_send()
        return carry

    ending.append(lambda: lax.fori_loop(0, sp_count, close, 0))
    ending.append(lambda: lax.fori_loop(1, sp_count, sent, 0))

    def expert(at, own):
        for s in at:
            ready(s)
        scales = [scale_of(s, o) for s, o in zip(at, own)]
        for e in range(local):
            inside = slice(e * capacity, (e + 1) * capacity)
            data = jnp.concatenate([rows_ref[s, inside, :] for s in at], axis=0)
            scale = jnp.concatenate([c[inside] for c in scales], axis=0)
            gate = dot(data, switch_ref[e]) * scale
            wide = dot(data, expand_ref[e]) * scale
            units = (gate / (1.0 + jnp.exp(-gate)) * wide).astype(BF16)
            value = dot(units, contract_ref[e]).astype(BF16)
            for c, s in enumerate(at):
                y_ref[s, inside, :] = value[c * capacity : (c + 1) * capacity]
        for s in at:
            for g in others:
                sib_copy(s, g).start()
            sib_copy(s, group).start()

    def meet(s):
        for g in others:
            sib_copy(s, g).wait_recv()
            for h, at in cuts:
                pair[s, g, at] = (
                    y_ref[s, at, span(g * 2 + core, cols)].astype(F32)
                    + from_sib[s, g, at].astype(F32)
                ).astype(BF16)
                peer_copy(s, g, h, at).start()

    def total_up(s, own):
        sib_copy(s, group).wait_recv()
        for h, at in cuts:
            total = y_ref[s, at, mine].astype(F32) + from_sib[s, group, at].astype(F32)
            for g in others:
                copy_to(
                    from_peer.at[s, g, at],
                    from_peer.at[s, g, at],
                    s_peer.at[s, g, h],
                    r_peer.at[s, g, h],
                    {"tp": g * 2 + core},
                ).wait_recv()
                total = total + from_peer[s, g, at].astype(F32)
            if own:
                back[s, at] = total.astype(BF16)
            else:
                summed[s, at] = total.astype(BF16)
                back_copy(s, h, at).start()

    def combine(s, own):
        if not own:
            for h, at in cuts:
                here = back.at[s, at]
                copy_to(here, here, s_back.at[s, h], r_back.at[s, h], {"sp": s}).wait_recv()
        chosen = [
            jnp.where(slots[k] == places + s * per, 1.0, 0.0).astype(BF16) for k in range(top)
        ]
        picked = dot(stack(*chosen), back[s])
        total = hidden_ref[...]
        for k in range(top):
            total = total + weights[k] * picked[k * rows : (k + 1) * rows]
        hidden_ref[...] = total

    return expert, meet, total_up, combine


def gather_out(tp_count, hidden_ref, out_ref, s_own, s_fwd, r_col):
    tp = lax.axis_index("tp")
    model = out_ref.shape[1]
    cols = model // tp_count
    mine = span(tp, cols)
    groups = tp_count // 2
    core, group = lax.rem(tp, 2), lax.div(tp, 2)
    sibling = group * 2 + 1 - core
    others = [lax.rem(group + d, groups) for d in range(1, groups)]
    out_ref[:, mine] = hidden_ref[...].astype(BF16)

    def own_copy(p):
        here = out_ref.at[:, mine]
        return copy_to(here, here, s_own.at[p], r_col.at[tp], {"tp": p})

    def forward(o):
        here = out_ref.at[:, span(o, cols)]
        return copy_to(here, here, s_fwd.at[o], r_col.at[o], {"tp": sibling})

    peers = [g * 2 + core for g in others]
    for p in peers:
        own_copy(p).start()
    own_copy(sibling).start()
    for p in peers:
        forward(p).wait_recv()
        forward(p).start()
    forward(sibling).wait_recv()
    for g in others:
        forward(g * 2 + 1 - core).wait_recv()
    own_copy(sibling).wait_send()
    for p in peers:
        own_copy(p).wait_send()
        forward(p).wait_send()


def plan(count, capacity):
    half = count // 2
    near, far = list(range(half)), list(range(half, count))
    if count == 8 and capacity == 128:
        return SENDS, SCRIPT
    chunk = max(1, 256 // capacity)
    steps = []
    for d in near + far:
        steps += [("R", d), ("F", d)]
    ranks = far + near[::-1]
    for i in range(0, count, chunk):
        steps.append(("E", *ranks[i : i + chunk]))
        steps += [("M", d) for d in ranks[i : i + chunk]]
        steps += [("T", d) for d in ranks[i : i + chunk]]
    return near[1:] + far, steps + [("C", d) for d in ranks]


def layer_kernel(
    head_dim, segment, sp_count, tp_count, experts, capacity,
    q_in, k_in, v_in, a_in, f_in, b_in, w_in, skip_in, switch_in, expand_in, contract_in,
    norm_in, gain_in, ids_in, chance_in, within_in,
    out_ref,
    q_ref, k_ref, v_ref, a_ref, f_ref, b_ref, w_ref, skip_ref,
    norm_ref, gain_ref, ids_ref, chance_ref, within_ref, s_in,
    local, maps_in, ka, got, fold, st, mixed,
    lent, kept, from_sib, pair, from_peer, squares, outgoing,
    s_map, r_map, s_fold, r_fold, s_sib, r_sib, s_peer, r_peer,
    s_sq, r_sq, s_out, r_out, s_own, s_fwd, r_col,
    hidden_ref, rows_ref, switch_ref, expand_ref, contract_ref,
    scale_out, scale_in, s_scale, r_scale, *back_refs,
):
    sp, tp = lax.axis_index("sp"), lax.axis_index("tp")
    rows, channels = q_in.shape
    model = skip_in.shape[1]
    cols = model // tp_count
    width = 2 * head_dim
    heads = channels // head_dim
    share = max(1, heads // sp_count)
    workers = heads // share
    mine = span(tp, cols)
    groups = tp_count // 2
    core, group = lax.rem(tp, 2), lax.div(tp, 2)
    sibling = group * 2 + 1 - core
    others = [lax.rem(group + g, groups) for g in range(1, groups)]
    early = [
        pltpu.make_async_copy(src, dst, s_in.at[i])
        for i, (src, dst) in enumerate(
            [(f_in, f_ref), (b_in, b_ref), (k_in, k_ref), (a_in, a_ref), (q_in, q_ref),
             (v_in, v_ref), (norm_in, norm_ref), (gain_in, gain_ref), (ids_in, ids_ref),
             (chance_in, chance_ref), (within_in, within_ref), (w_in, w_ref),
             (skip_in, skip_ref), (switch_in, switch_ref), (expand_in, expand_ref),
             (contract_in, contract_ref)]
        )
    ]
    for copy in early[:6]:
        copy.start()
    call_peers(sp_count, tp_count, sp, tp)
    for copy in early[:6]:
        copy.wait()
    for copy in early[6:]:
        copy.start()
    ending = []

    def unless_me(t, action):
        pl.when(t != sp)(action)

    def map_copy(t, owner):
        return copy_to(
            ka.at[pl.ds(t * share, share)], got.at[owner], s_map.at[t], r_map.at[owner], {"sp": t}
        )

    def fold_copy(t, owner):
        return copy_to(
            fold.at[t], st.at[pl.ds(owner * share, share)], s_fold.at[t], r_fold.at[owner], {"sp": t}
        )

    def emit_map(p, state):
        for h in range(2):
            part = slice(h * head_dim, (h + 1) * head_dim)
            ka[2 * p + h] = beside(state[:head_dim, part], state[head_dim:, part]).astype(BF16)

    def send_maps():
        meet_peers(sp_count, tp_count)
        if workers == sp_count:
            for d in range(1, sp_count):
                map_copy(mate(sp, d, sp_count), sp).start()
        else:
            for t in range(workers):
                unless_me(t, lambda t=t: map_copy(t, sp).start())

    def emit_rows(p, b, maps, out):
        at = (slice(b * segment, (b + 1) * segment), slice(p * width, (p + 1) * width))
        local[at] = out
        maps_in[at] = maps

    mixer_body(
        head_dim, segment, q_ref, k_ref, v_ref, a_ref, f_ref, b_ref, emit_map, send_maps, emit_rows
    )

    for copy in early[6:]:
        copy.wait()
    top = ids_ref.shape[0]
    within = within_ref[...]
    shares = chance_ref[...] * within / jnp.sum(within, axis=0, keepdims=True)
    lines = [ids_ref[k : k + 1, :].astype(F32) for k in range(top)]
    lines = lines + [shares[k : k + 1, :] for k in range(top)]
    place = lax.broadcasted_iota(jnp.int32, (8, rows), 0)
    table = jnp.zeros((8, rows), F32)
    for k in range(2 * top):
        table = jnp.where(place == k, lines[k], table)
    pieces = stack(*[piece.astype(F32) for piece in thirds(table)]).astype(BF16)
    unit = jnp.where(
        lax.rem(lax.broadcasted_iota(jnp.int32, (24, 128), 0), 8)
        == lax.broadcasted_iota(jnp.int32, (24, 128), 1),
        1.0,
        0.0,
    ).astype(BF16)
    upright = dot(pieces, unit, (0, 0))
    weights = [upright[:, top + k : top + k + 1] for k in range(top)]
    lanes = lax.broadcasted_iota(jnp.int32, (rows, experts), 1).astype(F32)
    named = [upright[:, k : k + 1] == lanes for k in range(top)]
    anyone = sum(jnp.where(n, 1.0, 0.0) for n in named).astype(BF16)
    r0 = lax.broadcasted_iota(jnp.int32, (rows, rows), 0)
    r1 = lax.broadcasted_iota(jnp.int32, (rows, rows), 1)
    before = dot(jnp.where(r0 > r1, 1.0, 0.0).astype(BF16), anyone)
    slots = [
        jnp.sum(
            jnp.where(n, before + lanes * capacity, 0.0), axis=1, keepdims=True
        ).astype(jnp.int32)
        for n in named
    ]
    def chain():
        got[sp] = ka[pl.ds(sp * share, share)]
        half = lax.div(lax.broadcasted_iota(jnp.int32, (head_dim, width), 1), head_dim)
        places = [half == lax.rem(sp * share + i, 2) for i in range(share)]
        state = [jnp.zeros((head_dim, head_dim), F32) for _ in range(share)]
        for j in range(sp_count):
            unless_me(
                j,
                lambda j=j: copy_to(
                    got.at[j], got.at[j], s_map.at[0], r_map.at[j], {"sp": j}
                ).wait_recv(),
            )
            for i in range(share):
                fold[j, i] = jnp.where(places[i], beside(state[i], state[i]), 0.0).astype(BF16)
            unless_me(j, lambda j=j: fold_copy(j, sp).start())
            for i in range(share):
                both = got[j, i]
                product = dot(stack(*halves(state[i])), both[:, :head_dim])
                state[i] = product[:head_dim] + product[head_dim:] + both[:, head_dim:].astype(F32)
        st[pl.ds(sp * share, share)] = fold[sp]

    def map_sent():
        for t in range(workers):
            unless_me(t, lambda t=t: map_copy(t, sp).wait_send())

    def fold_sent():
        for t in range(sp_count):
            unless_me(t, lambda t=t: fold_copy(t, sp).wait_send())

    ending.append(map_sent)
    ending.append(fold_sent if workers == sp_count else lambda: pl.when(sp < workers)(fold_sent))
    if workers == sp_count:
        chain()
    else:
        pl.when(sp < workers)(chain)
    ones = jnp.where(
        lax.div(lax.broadcasted_iota(jnp.int32, (width, width), 0), head_dim)
        == lax.div(lax.broadcasted_iota(jnp.int32, (width, width), 1), head_dim),
        1.0 / head_dim,
        0.0,
    ).astype(BF16)
    ones = stack(ones, ones)
    for t in range(workers):
        unless_me(
            t,
            lambda t=t: copy_to(
                fold.at[t], st.at[pl.ds(t * share, share)], s_fold.at[0], r_fold.at[t], {"sp": t}
            ).wait_recv(),
        )
    for p in range(heads // 2):
        part = slice(p * width, (p + 1) * width)
        states = stack(st[2 * p], st[2 * p + 1])
        output = local[:, part] + dot(maps_in[:, part], states, (1, 1))
        centered = output - dot(beside(*halves(output)), ones)
        spread = dot(beside(*halves(centered * centered)), ones)
        mixed[:, part] = (centered * lax.rsqrt(spread + 0.00064) * norm_ref[:, part]).astype(BF16)

    def sib_copy(g):
        return copy_to(lent.at[g], from_sib.at[g], s_sib.at[g], r_sib.at[g], {"tp": sibling})

    def peer_copy(g):
        return copy_to(
            pair.at[g], from_peer.at[group], s_peer.at[g], r_peer.at[group], {"tp": g * 2 + core}
        )

    ending.append(lambda: [sib_copy(g).wait_send() for g in others + [group]])
    ending.append(lambda: [peer_copy(g).wait_send() for g in others])
    for g in others + [group]:
        lent[g] = dot(mixed[...], w_ref[:, span(g * 2 + 1 - core, cols)]).astype(BF16)
        sib_copy(g).start()
    for g in others + [group]:
        kept[g] = dot(mixed[...], w_ref[:, span(g * 2 + core, cols)])
    for g in others:
        sib_copy(g).wait_recv()
        pair[g] = (kept[g] + from_sib[g].astype(F32)).astype(BF16)
        peer_copy(g).start()
    sib_copy(group).wait_recv()
    hidden = skip_ref[:, mine].astype(F32) + (kept[group] + from_sib[group].astype(F32))
    for g in others:
        copy_to(
            pair.at[g], from_peer.at[g], s_peer.at[g], r_peer.at[g], {"tp": g * 2 + core}
        ).wait_recv()
        hidden = hidden + from_peer[g].astype(F32)
    hidden_ref[...] = hidden
    squares[tp] = row_total(hidden * hidden, 3)

    def square_copy(p):
        return copy_to(squares.at[tp], squares.at[tp], s_sq.at[p], r_sq.at[tp], {"tp": p})

    ending.append(
        lambda: [square_copy(lax.rem(tp + d, tp_count)).wait_send() for d in range(1, tp_count)]
    )
    for d in range(1, tp_count):
        square_copy(lax.rem(tp + d, tp_count)).start()
    normed = (hidden * gain_ref[:, mine]).astype(BF16)

    per = experts // sp_count * capacity
    places = lax.broadcasted_iota(jnp.int32, (rows, per), 1)

    def chosen_for(t):
        at = places + t * per
        chosen = slots[0] == at
        for s in slots[1:]:
            chosen = chosen | (s == at)
        return jnp.where(chosen, 1.0, 0.0).astype(BF16)

    def block_for(t):
        return dot(chosen_for(t), normed, (0, 0)).astype(BF16)

    cuts = cuts_of(per)

    def out_copy(t, h, at):
        return copy_to(
            outgoing.at[t, at], rows_ref.at[sp, at, mine], s_out.at[t, h], r_out.at[sp, h], {"sp": t}
        )

    def own_copy(p, s, h, at):
        here = rows_ref.at[s, at, mine]
        return copy_to(here, here, s_own.at[p, s, h], r_col.at[tp, s, h], {"tp": p})

    def forward(o, s, h, at):
        here = rows_ref.at[s, at, span(o, cols)]
        return copy_to(here, here, s_fwd.at[o, s, h], r_col.at[o, s, h], {"tp": sibling})

    peers = [g * 2 + core for g in others]

    def pass_on(s, arrival=None):
        for cut in cuts:
            if arrival is not None:
                arrival(*cut).wait_recv()
            for p in peers:
                own_copy(p, s, *cut).start()
            own_copy(sibling, s, *cut).start()

    def settle(s, carry):
        for cut in cuts:
            own_copy(sibling, s, *cut).wait_send()
            for p in peers:
                own_copy(p, s, *cut).wait_send()
                forward(p, s, *cut).wait_send()
        return carry

    def sent(d, carry):
        for cut in cuts:
            out_copy(lax.rem(sp + d, sp_count), *cut).wait_send()
        return carry

    ending.append(lambda: lax.fori_loop(0, sp_count, settle, 0))
    ending.append(lambda: lax.fori_loop(1, sp_count, sent, 0))

    def ready(s):
        for cut in cuts:
            forward(sibling, s, *cut).wait_recv()
            for g in others:
                forward(g * 2 + 1 - core, s, *cut).wait_recv()

    sends, steps = plan(sp_count, capacity)

    def source(d):
        return mate(sp, d, sp_count)

    y_ref, sib_back, pair_back, peer_back, summed, returned = back_refs[:6]
    s_sib2, r_sib2, s_peer2, r_peer2, s_back, r_back, s_last, s_fwd2, r_last = back_refs[6:]
    for d in sends:
        t = mate(sp, d, sp_count)
        outgoing[t] = block_for(t)
        for cut in cuts:
            out_copy(t, *cut).start()
    rows_ref[sp, :, mine] = block_for(sp)
    total = squares[tp]
    for d in range(1, tp_count):
        p = lax.rem(tp + d, tp_count)
        copy_to(squares.at[p], squares.at[p], s_sq.at[p], r_sq.at[p], {"tp": p}).wait_recv()
        total = total + squares[p]
    inverse = [piece.astype(F32) for piece in thirds(lax.rsqrt(total / model + 1e-06))]
    inverse = stack(*inverse).astype(BF16)

    def scale_for(t):
        product = dot(inverse, chosen_for(t))
        return product[:8] + product[8:16] + product[16:]

    def scale_copy(t):
        return copy_to(
            scale_out.at[t], scale_in.at[sp], s_scale.at[t], r_scale.at[sp], {"sp": t}
        )

    def scale_sent(d, carry):
        scale_copy(lax.rem(sp + d, sp_count)).wait_send()
        return carry

    ending.append(lambda: lax.fori_loop(1, sp_count, scale_sent, 0))
    for d in sends:
        t = mate(sp, d, sp_count)
        scale_out[t] = scale_for(t)
        scale_copy(t).start()
    scale_in[sp] = scale_for(sp)
    one = jnp.where(
        lax.rem(lax.broadcasted_iota(jnp.int32, (24, 128), 0), 8) == 0, 1.0, 0.0
    ).astype(BF16)

    def scale_of(s, own):
        if not own:
            copy_to(
                scale_in.at[s], scale_in.at[s], s_scale.at[s], r_scale.at[s], {"sp": s}
            ).wait_recv()
        pieces = stack(*[piece.astype(F32) for piece in thirds(scale_in[s])]).astype(BF16)
        return dot(pieces, one, (0, 0))[:, :1]

    expert, meet, total_up, combine = experts_back(
        sp_count, tp_count, ready, scale_of,
        rows_ref, switch_ref, expand_ref, contract_ref, hidden_ref, slots, weights,
        y_ref, sib_back, pair_back, peer_back, summed, returned,
        s_sib2, r_sib2, s_peer2, r_peer2, s_back, r_back, ending,
    )
    for kind, *which in steps:
        for d in which[:1] if kind == "E" else which:
            s = source(d)
            if kind == "R" and d:

                def arrival(h, at, s=s):
                    here = rows_ref.at[s, at, mine]
                    return copy_to(here, here, s_out.at[s, h], r_out.at[s, h], {"sp": s})

                pass_on(s, arrival)
            if kind == "R" and not d:
                pass_on(s)
            if kind == "F":
                for cut in cuts:
                    for o in peers:
                        forward(o, s, *cut).wait_recv()
                        forward(o, s, *cut).start()
            if kind == "E":
                expert([source(i) for i in which], [i == 0 for i in which])
            if kind == "M":
                meet(s)
            if kind == "T":
                total_up(s, d == 0)
            if kind == "C":
                combine(s, d == 0)
    gather_out(tp_count, hidden_ref, out_ref, s_last, s_fwd2, r_last)
    for wait in ending:
        wait()


def body(
    readout_query_vectors,
    attention_key_vectors,
    attention_content_vectors,
    step_size_preactivation,
    forgetting_preactivation,
    extra_forgetting_bias,
    subspace_normalizer_gain,
    skip_connection_stream,
    blender_projection_matrix,
    specialist_prenormal_gain,
    cluster_router_chance,
    specialist_chance_within_cluster,
    chosen_specialist_ids,
    specialist_switch_matrix,
    specialist_expansion_matrix,
    specialist_contraction_matrix,
):
    tok_rows, model_width = skip_connection_stream.shape
    sp_count, tp_count = lax.axis_size("sp"), lax.axis_size("tp")
    local_experts = specialist_switch_matrix.shape[0]
    experts = local_experts * sp_count
    top_count = chosen_specialist_ids.shape[1]
    capacity = 2 * tok_rows * top_count // experts
    cols = model_width // tp_count
    per = local_experts * capacity
    groups = tp_count // 2
    pieces = len(cuts_of(per))
    channels = readout_query_vectors.shape[1]
    heads = extra_forgetting_bias.shape[1]
    head_dim = channels // heads
    share = max(1, heads // sp_count)
    vmem = pl.BlockSpec(memory_space=pltpu.VMEM)
    hbm = pl.BlockSpec(memory_space=pltpu.HBM)
    sems = pltpu.SemaphoreType.DMA
    return pl.pallas_call(
        functools.partial(
            layer_kernel, head_dim, min(64, tok_rows), sp_count, tp_count, experts, capacity
        ),
        out_shape=jax.ShapeDtypeStruct((tok_rows, model_width), BF16),
        in_specs=[hbm] * 16,
        out_specs=vmem,
        scratch_shapes=[
            pltpu.VMEM((tok_rows, channels), BF16),
            pltpu.VMEM((tok_rows, channels), BF16),
            pltpu.VMEM((tok_rows, channels), BF16),
            pltpu.VMEM((tok_rows, channels), BF16),
            pltpu.VMEM((tok_rows, channels), F32),
            pltpu.VMEM((heads, tok_rows), F32),
            pltpu.VMEM((channels, model_width), BF16),
            pltpu.VMEM((tok_rows, model_width), BF16),
            pltpu.VMEM((1, channels), F32),
            pltpu.VMEM((1, model_width), F32),
            pltpu.VMEM((top_count, tok_rows), jnp.int32),
            pltpu.VMEM((1, tok_rows), F32),
            pltpu.VMEM((top_count, tok_rows), F32),
            sems((16,)),
            pltpu.VMEM((tok_rows, channels), F32),
            pltpu.VMEM((tok_rows, channels), BF16),
            pltpu.VMEM((heads, head_dim, 2 * head_dim), BF16),
            pltpu.VMEM((sp_count, share, head_dim, 2 * head_dim), BF16),
            pltpu.VMEM((sp_count, share, head_dim, 2 * head_dim), BF16),
            pltpu.VMEM((heads, head_dim, 2 * head_dim), BF16),
            pltpu.VMEM((tok_rows, channels), BF16),
            pltpu.VMEM((groups, tok_rows, cols), BF16),
            pltpu.VMEM((groups, tok_rows, cols), F32),
            pltpu.VMEM((groups, tok_rows, cols), BF16),
            pltpu.VMEM((groups, tok_rows, cols), BF16),
            pltpu.VMEM((groups, tok_rows, cols), BF16),
            pltpu.VMEM((tp_count, 8, tok_rows), F32),
            pltpu.VMEM((sp_count, per, cols), BF16),
            sems((sp_count,)),
            sems((sp_count,)),
            sems((sp_count,)),
            sems((sp_count,)),
            sems((groups,)),
            sems((groups,)),
            sems((groups,)),
            sems((groups,)),
            sems((tp_count,)),
            sems((tp_count,)),
            sems((sp_count, pieces)),
            sems((sp_count, pieces)),
            sems((tp_count, sp_count, pieces)),
            sems((tp_count, sp_count, pieces)),
            sems((tp_count, sp_count, pieces)),
            pltpu.VMEM((tok_rows, cols), F32),
            pltpu.VMEM((sp_count, per, model_width), BF16),
            pltpu.VMEM(specialist_switch_matrix.shape, BF16),
            pltpu.VMEM(specialist_expansion_matrix.shape, BF16),
            pltpu.VMEM(specialist_contraction_matrix.shape, BF16),
            pltpu.VMEM((sp_count, 8, per), F32),
            pltpu.VMEM((sp_count, 8, per), F32),
            sems((sp_count,)),
            sems((sp_count,)),
            pltpu.VMEM((sp_count, per, model_width), BF16),
            pltpu.VMEM((sp_count, groups, per, cols), BF16),
            pltpu.VMEM((sp_count, groups, per, cols), BF16),
            pltpu.VMEM((sp_count, groups, per, cols), BF16),
            pltpu.VMEM((sp_count, per, cols), BF16),
            pltpu.VMEM((sp_count, per, cols), BF16),
            sems((sp_count, groups)),
            sems((sp_count, groups)),
            sems((sp_count, groups, pieces)),
            sems((sp_count, groups, pieces)),
            sems((sp_count, pieces)),
            sems((sp_count, pieces)),
            sems((tp_count,)),
            sems((tp_count,)),
            sems((tp_count,)),
        ],
        compiler_params=pltpu.CompilerParams(
            collective_id=1, has_side_effects=True, vmem_limit_bytes=VMEM_LIMIT
        ),
    )(
        *[
            pltpu.with_memory_space_constraint(operand, pltpu.HBM)
            for operand in (
                readout_query_vectors,
                attention_key_vectors,
                attention_content_vectors,
                step_size_preactivation,
                forgetting_preactivation,
                extra_forgetting_bias.T,
                blender_projection_matrix,
                skip_connection_stream,
                specialist_switch_matrix,
                specialist_expansion_matrix,
                specialist_contraction_matrix,
                subspace_normalizer_gain.reshape(1, channels),
                specialist_prenormal_gain.reshape(1, model_width),
                chosen_specialist_ids.T,
                cluster_router_chance.reshape(1, tok_rows),
                specialist_chance_within_cluster.T,
            )
        ]
    )


def solution(mesh):
    in_specs = (
        P("sp", "tp"),
        P("sp", "tp"),
        P("sp", "tp"),
        P("sp", "tp"),
        P("sp", "tp"),
        P("sp", "tp"),
        P("tp"),
        P("sp", None),
        P("tp", None),
        P(),
        P("sp"),
        P("sp", None),
        P("sp", None),
        P("sp", None, "tp"),
        P("sp", None, "tp"),
        P("sp", "tp", None),
    )
    out_specs = P("sp", None)
    return jax.shard_map(body, mesh=mesh, in_specs=in_specs, out_specs=out_specs, check_vma=False)
```
